256 devices in a mesh: sp: 64 (over z, y, core), tp: 4 (over x).
Axes of the slice: x: 4, y: 4, z: 8, core: 2. Of those that a mesh axis runs over, the one named last changes fastest.
Arguments:
- resid: bfloat16 [12288, 2048], P('sp'), may hold values from -6 to 6
- query_broad: bfloat16 [12288, 1536], P('sp', 'tp'), may hold values from -60 to 60
- query_narrow: bfloat16 [12288, 1024], P('sp', 'tp'), may hold values from -60 to 60
- latent: bfloat16 [12288, 512], P('sp'), may hold values from -6 to 6
- key_rope: bfloat16 [12288, 64], P('sp'), may hold values from -6 to 6
- latent_gain: float32 [512], replicated, may hold values from 0.1 to 1.9
- key_up_broad: bfloat16 [512, 1024], P(None, 'tp'), may hold values from -0.25 to 0.25
- value_up_broad: bfloat16 [512, 1024], P(None, 'tp'), may hold values from -0.25 to 0.25
- key_up_narrow: bfloat16 [512, 512], P(None, 'tp'), may hold values from -0.25 to 0.25
- value_up_narrow: bfloat16 [512, 512], P(None, 'tp'), may hold values from -0.25 to 0.25
- out_broad: bfloat16 [1024, 2048], replicated, may hold values from -0.15625 to 0.15625
- out_narrow: bfloat16 [512, 2048], replicated, may hold values from -0.15625 to 0.15625
- post_gain: float32 [2048], replicated, may hold values from 0.1 to 1.9
- ffn_gain: float32 [2048], replicated, may hold values from 0.1 to 1.9
- up_weight: bfloat16 [2048, 8192], P('sp', 'tp'), may hold values from -0.125 to 0.125
- down_weight: bfloat16 [2048, 8192], P('sp', 'tp'), may hold values from -0.0625 to 0.0625
- ffn_out_gain: float32 [2048], replicated, may hold values from 0.1 to 1.9
Outputs:
- layer_out: bfloat16 [12288, 2048], P(('sp', 'tp'))
The draws below stay inside these ranges and needn't reach their ends.
All inputs are finite; a program needn't handle non-finite values.
Results may differ from the reference program's by a relative error of at most 0.013.
Values may be sent and summed in bfloat16 or wider, within the bound.
A program may use at most 128 MiB of HBM per device.

```python
import math
import jax
import jax.numpy as jnp
from jax import lax

D = 2048
FF = 8192
R = 512
ROPE = 64
DB = 128
DN = 64
HB = 8
HN = 8
SEQ = 12288


def drawn_queries(key, salt, head_count, head_size):
    drawn = jax.random.normal(jax.random.fold_in(key, salt), (SEQ, head_count, head_size + ROPE), jnp.float32)
    return jnp.clip(drawn, -6.0, 6.0)


def draw_query_broad(key, part):
    entries = drawn_queries(key, 21, HB, DB)
    return entries.reshape(SEQ, HB * (DB + ROPE)).astype(jnp.bfloat16)


def draw_query_narrow(key, part):
    entries = drawn_queries(key, 31, HN, DN)
    return entries.reshape(SEQ, HN * (DN + ROPE)).astype(jnp.bfloat16)


def draw_key_rope(key, part):
    entries = jnp.clip(jax.random.normal(jax.random.fold_in(key, 11), (SEQ, ROPE), jnp.float32), -6.0, 6.0)
    return entries.astype(jnp.bfloat16)


def block_scale(rng, dims, cuts, least, top_value):
    def one(dim, shards_of):
        heights = jax.random.uniform(jax.random.fold_in(jax.random.fold_in(rng, 6), dim), (shards_of,), jnp.float32, least / len(cuts), top_value / len(cuts))
        return jnp.repeat(jnp.exp(heights), dims[dim] // shards_of).reshape((-1,) + (1,) * (len(dims) - dim - 1))

    factor_of = one(*cuts[0])
    for cut in cuts[1:]:
        factor_of = factor_of * one(*cut)
    return factor_of


def bell_draw(rng, extent, width, reach, cuts=(), held_as=jnp.bfloat16):
    factor_of = block_scale(rng, extent, cuts, -0.22, 0.18) if cuts else 1.0
    result = jax.random.normal(rng, extent, jnp.float32) * width * factor_of
    return jnp.minimum(jnp.maximum(result, -reach), reach).astype(held_as)


def setup_inputs(seed: int = 0) -> dict:
    streams_of = jax.random.split(jax.random.key(seed), 18)
    return {
        "resid": bell_draw(streams_of[0], (SEQ, D), 1.0, 6.0, ((0, 64),)),
        "query_broad": draw_query_broad(jax.random.fold_in(streams_of[17], 71), 0),
        "query_narrow": draw_query_narrow(jax.random.fold_in(streams_of[17], 71), 0),
        "latent": bell_draw(streams_of[3], (SEQ, R), 1.0, 6.0, ((0, 64),)),
        "key_rope": draw_key_rope(jax.random.fold_in(streams_of[17], 71), 0),
        "latent_gain": jnp.clip(1.0 + 0.18 * jax.random.normal(streams_of[5], (R,), jnp.float32), 0.1, 1.9),
        "key_up_broad": bell_draw(streams_of[6], (R, HB * DB), R ** -0.5, 0.25, ((1, 4),)),
        "value_up_broad": bell_draw(streams_of[7], (R, HB * DB), R ** -0.5, 0.25, ((1, 4),)),
        "key_up_narrow": bell_draw(streams_of[8], (R, HN * DN), R ** -0.5, 0.25, ((1, 4),)),
        "value_up_narrow": bell_draw(streams_of[9], (R, HN * DN), R ** -0.5, 0.25, ((1, 4),)),
        "out_broad": bell_draw(streams_of[10], (HB * DB, D), (HB * DB + HN * DN) ** -0.5, 0.15625),
        "out_narrow": bell_draw(streams_of[11], (HN * DN, D), (HB * DB + HN * DN) ** -0.5, 0.15625),
        "post_gain": jnp.clip(1.0 + 0.18 * jax.random.normal(streams_of[12], (D,), jnp.float32), 0.1, 1.9),
        "ffn_gain": jnp.clip(1.0 + 0.18 * jax.random.normal(streams_of[13], (D,), jnp.float32), 0.1, 1.9),
        "up_weight": bell_draw(streams_of[14], (D, FF), D ** -0.5, 0.125, ((0, 64), (1, 4))),
        "down_weight": bell_draw(streams_of[15], (D, FF), FF ** -0.5, 0.0625, ((0, 64), (1, 4))),
        "ffn_out_gain": jnp.clip(1.0 + 0.18 * jax.random.normal(streams_of[16], (D,), jnp.float32), 0.1, 1.9),
    }


norm_eps = 1e-06
rope_base = 500000.0
masked_score = -1e+30

def rotate(values, positions):
    full_width = values.shape[-1]
    half_width = full_width // 2
    frequency = rope_base ** (-2.0 * jnp.arange(half_width, dtype=jnp.float32) / full_width)
    angles = positions.astype(jnp.float32)[:, None] * frequency[None, :]
    angle_shape = (angles.shape[0],) + (1,) * (values.ndim - 2) + (half_width,)
    cosine = jnp.cos(angles).reshape(angle_shape)
    sine_part = jnp.sin(angles).reshape(angle_shape)
    leading = values[..., :half_width]
    trailing = values[..., half_width:]
    return jnp.concatenate([leading * cosine - trailing * sine_part, trailing * cosine + leading * sine_part], axis=-1)

def rms_scale(values, norm_gain):
    return values * lax.rsqrt(lax.optimization_barrier(jnp.mean(values * values, axis=-1, keepdims=True)) + norm_eps) * norm_gain

def attend_all(query_nope, query_rope, key_rows, key_rot, value_rows, score_scale):
    block_rows = math.gcd(SEQ, 512)
    positions = jnp.arange(SEQ, dtype=jnp.int32)
    keys_wide = key_rows.astype(jnp.float32)
    rot_wide = key_rot.astype(jnp.float32)
    values_wide = value_rows.astype(jnp.float32)

    def one_block(block_index):
        begin = block_index * block_rows
        nope_part = lax.dynamic_slice_in_dim(query_nope, begin, block_rows, 0).astype(jnp.float32)
        rope_part = lax.dynamic_slice_in_dim(query_rope, begin, block_rows, 0).astype(jnp.float32)
        query_pos = begin + jnp.arange(block_rows, dtype=jnp.int32)
        scores = jnp.einsum('qhd,khd->hqk', nope_part, keys_wide) + jnp.einsum('qhd,kd->hqk', rope_part, rot_wide)
        scores = scores * score_scale
        allowed = (positions[None, :] <= query_pos[:, None])[None]
        scores = jnp.where(allowed, scores, masked_score)
        highest = lax.optimization_barrier(jnp.max(scores, axis=-1, keepdims=True))
        exponent = jnp.where(allowed, jnp.exp(scores - highest), 0.0)
        denominator = lax.optimization_barrier(jnp.sum(exponent, axis=-1))
        rounded = lax.optimization_barrier(exponent.astype(jnp.bfloat16)).astype(jnp.float32)
        summed = jnp.einsum('hqk,khd->qhd', rounded, values_wide)
        return (summed / jnp.transpose(denominator)[:, :, None]).astype(jnp.bfloat16)
    heads_out = lax.map(one_block, jnp.arange(SEQ // block_rows, dtype=jnp.int32))
    return heads_out.reshape(SEQ, value_rows.shape[1] * value_rows.shape[2])

def reference(resid, query_broad, query_narrow, latent, key_rope, latent_gain, key_up_broad, value_up_broad, key_up_narrow, value_up_narrow, out_broad, out_narrow, post_gain, ffn_gain, up_weight, down_weight, ffn_out_gain):
    positions = jnp.arange(SEQ, dtype=jnp.int32)
    latent_normed = rms_scale(latent.astype(jnp.float32), latent_gain).astype(jnp.bfloat16)

    def expand(weight, head_size):
        product = jnp.dot(latent_normed, weight, preferred_element_type=jnp.float32)
        return product.astype(jnp.bfloat16).reshape(SEQ, -1, head_size)
    key_broad = expand(key_up_broad, DB)
    value_broad = expand(value_up_broad, DB)
    key_narrow = expand(key_up_narrow, DN)
    value_narrow = expand(value_up_narrow, DN)
    key_rot = rotate(key_rope.astype(jnp.float32), positions).astype(jnp.bfloat16)
    broad_heads = query_broad.reshape(SEQ, HB, DB + ROPE)
    broad_rope = rotate(broad_heads[:, :, DB:].astype(jnp.float32), positions).astype(jnp.bfloat16)
    narrow_heads = query_narrow.reshape(SEQ, HN, DN + ROPE)
    narrow_rope = rotate(narrow_heads[:, :, DN:].astype(jnp.float32), positions).astype(jnp.bfloat16)
    attn_broad = attend_all(broad_heads[:, :, :DB], broad_rope, key_broad, key_rot, value_broad, (DB + ROPE) ** (-0.5))
    attn_narrow = attend_all(narrow_heads[:, :, :DN], narrow_rope, key_narrow, key_rot, value_narrow, (DN + ROPE) ** (-0.5))
    projected = jnp.dot(attn_broad, out_broad, preferred_element_type=jnp.float32) + jnp.dot(attn_narrow, out_narrow, preferred_element_type=jnp.float32)
    mixed = (resid.astype(jnp.float32) + rms_scale(projected, post_gain)).astype(jnp.bfloat16)
    normed = rms_scale(mixed.astype(jnp.float32), ffn_gain).astype(jnp.bfloat16)
    hidden = jnp.square(jax.nn.relu(jnp.dot(normed, up_weight, preferred_element_type=jnp.float32))).astype(jnp.bfloat16)
    ffn = lax.dot_general(hidden, down_weight, (((1,), (1,)), ((), ())), preferred_element_type=jnp.float32)
    return (mixed.astype(jnp.float32) + rms_scale(ffn, ffn_out_gain)).astype(jnp.bfloat16)
```

```python
import functools
import math

import jax
import jax.numpy as jnp
from jax import lax
from jax.experimental import pallas as pl
from jax.experimental.pallas import tpu as pltpu
from jax.sharding import PartitionSpec as P

DB = 128
DN = 64
ROPE = 64
NY = 4

norm_eps = 1e-06
rope_base = 500000.0
broad_unit = (DB + ROPE) ** (-0.5) * math.log2(math.e)
narrow_unit = (DN + ROPE) ** (-0.5) * math.log2(math.e)
f32 = jnp.float32
bf16 = jnp.bfloat16


def dot(a, b, dims=((1,), (0,))):
    return lax.dot_general(a, b, (dims, ((), ())), preferred_element_type=f32)


def picker(shape, pick):
    rows = lax.broadcasted_iota(jnp.int32, shape, 0)
    columns = lax.broadcasted_iota(jnp.int32, shape, 1)
    return jnp.where(pick(rows, columns), 1.0, 0.0).astype(bf16)


LAST = ((1,), (1,))


def prepare(core, q_broad, q_narrow, cosines, sines, refs, qt_broad, qt_narrow, w_key, w_value_t):
    key_up_broad, value_up_broad, key_up_narrow, value_up_narrow = refs
    at = core * (DB + ROPE)
    rows = q_broad.shape[0]
    wide = q_broad.shape[1]
    qt_broad[0:DB] = dot(
        picker((DB, wide), lambda r, k: k == r + at), q_broad, LAST
    ).astype(bf16)
    qt_broad[DB : DB + 64] = jnp.zeros((64, rows), bf16)

    def rotated(value, start):
        straight = dot(picker((64, value.shape[1]), lambda r, k: k == r + start), value, LAST)
        swapped = dot(
            picker(
                (64, value.shape[1]), lambda r, k: k == jnp.where(r < 32, r + 32, r - 32) + start
            ),
            value,
            LAST,
        )
        return (straight * cosines + swapped * sines).astype(bf16)

    qt_broad[DB + 64 : DB + 128] = rotated(q_broad, at + DB)
    at_n = core * (DN + ROPE)
    qt_narrow[0:64] = dot(
        picker((64, q_narrow.shape[1]), lambda r, k: k == r + at_n), q_narrow, LAST
    ).astype(bf16)
    qt_narrow[64:128] = rotated(q_narrow, at_n + DN)
    w_key[:, 0:DB] = key_up_broad[:, pl.ds(pl.multiple_of(core * DB, DB), DB)]
    w_key[:, DB : DB + 128] = dot(
        key_up_narrow[...], picker((128, 128), lambda r, k: (r == k + core * DN) & (k < DN))
    ).astype(bf16)
    w_value_t[0:DB] = dot(
        picker((DB, 2 * DB), lambda r, k: k == r + core * DB), value_up_broad[...], LAST
    ).astype(bf16)
    w_value_t[DB : DB + DN] = dot(
        picker((DN, 2 * DN), lambda r, k: k == r + core * DN), value_up_narrow[...], LAST
    ).astype(bf16)


def attend_block(block, diagonal, qt_broad, qt_narrow, w_key, w_value_t, top, total, acc):
    keys, queries = block.shape[0], qt_broad.shape[1]
    latent = block[:, 0:512]
    expanded = dot(latent, w_key[...])
    key_b = expanded[:, 0:DB].astype(bf16)
    key_n = (expanded[:, DB : DB + 128] + block[:, 512:640].astype(f32)).astype(bf16)
    value_t = dot(w_value_t[...], latent, LAST).astype(bf16)
    score_b = dot(jnp.concatenate([key_b, key_n], axis=1), qt_broad[...])
    score_n = dot(key_n, qt_narrow[...])
    if diagonal:
        allowed = lax.broadcasted_iota(jnp.int32, (keys, queries), 0) <= lax.broadcasted_iota(
            jnp.int32, (keys, queries), 1
        )
    for head, (score, unit, start, size) in enumerate(
        ((score_b, broad_unit, 0, DB), (score_n, narrow_unit, DB, DN))
    ):
        if diagonal:
            score = jnp.where(allowed, score, -1e30)
            peak = jnp.max(score, axis=0, keepdims=True)
        else:
            peak = jnp.maximum(top[head], jnp.max(score, axis=0, keepdims=True))
        weight = jnp.exp2((score - peak) * unit)
        if diagonal:
            weight = jnp.where(allowed, weight, 0.0)
        added = jnp.sum(weight, axis=0, keepdims=True)
        product = dot(value_t[start : start + size], weight.astype(bf16))
        if diagonal:
            total[head] = added
            acc[start : start + size] = product
        else:
            factor = jnp.exp2((top[head] - peak) * unit)
            total[head] = total[head] * factor + added
            acc[start : start + size] = acc[start : start + size] * factor + product
        top[head] = peak


def ring_places(axis_size):
    return lambda at, step: lax.rem(at + step + axis_size, axis_size)


class Spread:
    def __init__(self, held, sent, arrived, place, first, first_cut, rest_cut):
        self.held, self.sent, self.arrived = held, sent, arrived
        self.z, self.y, self.core = place
        self.nz, self.ny, _, self.rows, _ = held.shape
        self.first, self.first_cut, self.rest_cut = first, first_cut, rest_cut
        self.half_z, self.half_y = self.nz // 2, self.ny // 2
        names = [("ay", s, d) for s in (0, 1) for d in (1, -1)]
        for s in range(self.half_z):
            for d in (1, -1):
                names.append(("bz", s, d))
                for ch in (0, 1):
                    if s < self.half_z - 1 or ch == (0 if d == 1 else 1):
                        names.append(("az", s, d, ch))
                        names.append(("pa", s, d, ch))
        for s in (0, 1):
            for d in (1, -1):
                for ch in (0, 1):
                    if s == 0 or ch == (0 if d == 1 else 1):
                        names.append(("by", s, d, ch))
                        names.append(("pb", s, d, ch))
        names += [("pa", -1, 1, 0), ("pa", -1, 1, 1), ("pb", -1, 1, 0)]
        self.index = {name: i for i, name in enumerate(names)}

    @staticmethod
    def count(nz, ny):
        return 4 + (nz // 2) * 2 + 2 * ((nz // 2 - 1) * 4 + 2) + 2 * 6 + 3

    def device(self, z, y, core):
        return {"sp": (z * self.ny + y) * 2 + core}

    def copy(self, name):
        kind, s, d = name[:3]
        zs, ys = ring_places(self.nz), ring_places(self.ny)
        z, y, c, held, first = self.z, self.y, self.core, self.held, self.first
        low, high = pl.ds(0, first), pl.ds(first, self.rows - first)
        i = self.index[name]
        if kind == "ay":
            if s == 1:
                low = (
                    pl.ds(0, self.first_cut)
                    if d == 1
                    else pl.ds(self.first_cut, first - self.first_cut)
                )
            view, to = held.at[z, ys(y, -s * d), c, low], self.device(z, ys(y, d), c)
        elif kind == "bz":
            if s == self.half_z - 1:
                high = (
                    pl.ds(first, self.rest_cut)
                    if d == 1
                    else pl.ds(first + self.rest_cut, self.rows - first - self.rest_cut)
                )
            view, to = held.at[zs(z, -s * d), y, c, high], self.device(zs(z, d), y, c)
        elif kind == "az":
            part = pl.ds(name[3] * self.half_y, self.half_y)
            view, to = held.at[zs(z, -s * d), part, c, low], self.device(zs(z, d), y, c)
        elif kind == "by":
            part = pl.ds(name[3] * self.half_z, self.half_z)
            view, to = held.at[part, ys(y, -s * d), c, high], self.device(z, ys(y, d), c)
        elif kind == "pa":
            part = pl.ds(name[3] * self.half_y, self.half_y)
            view, to = held.at[zs(z, -(s + 1) * d), part, c, low], self.device(z, y, 1 - c)
        else:
            part = pl.ds(0, self.nz) if s == -1 else pl.ds(name[3] * self.half_z, self.half_z)
            view, to = held.at[part, ys(y, -(s + 1) * d), c, high], self.device(z, y, 1 - c)
        return pltpu.make_async_remote_copy(
            src_ref=view,
            dst_ref=view,
            send_sem=self.sent.at[i],
            recv_sem=self.arrived.at[i],
            device_id=to,
            device_id_type=pl.DeviceIdType.MESH,
        )

    def start(self, *names):
        for name in names:
            self.copy(name).start()

    def landed(self, *names):
        for name in names:
            self.copy(name).wait_recv()

    def both(self, kind, s):
        return [n for n in self.index if n[0] == kind and n[1] == s]

    def begin(self):
        self.start(*self.both("ay", 0), *self.both("bz", 0))

    def open_rings(self):
        self.landed(*self.both("ay", 0))
        self.start(*self.both("ay", 1))
        self.landed(*self.both("bz", 0))
        self.start(*self.both("bz", 1))
        self.landed(*self.both("ay", 1))
        self.start(*self.both("az", 0), *self.both("pa", -1))
        for s in range(1, self.half_z):
            self.landed(*self.both("bz", s))
            if s + 1 < self.half_z:
                self.start(*self.both("bz", s + 1))
        self.start(*self.both("by", 0), *self.both("pb", -1))

    def pass_on(self, name):
        kind, s, d, ch = name
        self.landed(name)
        following = (kind, s + 1, d, ch)
        if following in self.index:
            self.start(following)
        self.start(("p" + kind[0], s, d, ch))

    def order(self):
        names = []
        for s in range(self.half_z):
            if s == self.half_z // 2:
                names += self.both("by", 0)
            if s == self.half_z - 1:
                names += self.both("by", 1)
            names += self.both("az", s)
        return names

    def own_chip(self):
        return [*self.both("pa", -1), *self.both("pb", -1)]

    def handed(self):
        return [n for n in self.index if n[0] in ("pa", "pb") and n[1] >= 0]

    def drain(self):
        for name in self.index:
            self.copy(name).wait_send()


def attention_kernel(
    geometry,
    rows_hbm,
    q_broad,
    q_narrow,
    cosines,
    sines,
    key_up_broad,
    value_up_broad,
    key_up_narrow,
    value_up_narrow,
    out,
    held,
    all_q_broad,
    all_q_narrow,
    qt_broad,
    qt_narrow,
    w_key,
    w_value_t,
    top,
    total,
    acc,
    finished,
    own_sem,
    sent,
    arrived,
    more_sent,
    more_arrived,
):
    nz, ny, first, first_cut, rest_cut = geometry
    me = lax.axis_index("sp")
    core = lax.rem(me, 2)
    chip = me // 2
    z, y = chip // ny, lax.rem(chip, ny)
    rows = rows_hbm.shape[0]
    zs, ys = ring_places(nz), ring_places(ny)
    spread = Spread(held, sent, arrived, (z, y, core), first, first_cut, rest_cut)

    own = pltpu.make_async_copy(rows_hbm, held.at[z, y, core], own_sem)
    own.start()
    barrier = pltpu.get_barrier_semaphore()
    neighbours = [
        spread.device(z, y, 1 - core),
        spread.device(z, ys(y, 1), core),
        spread.device(z, ys(y, -1), core),
        spread.device(zs(z, 1), y, core),
        spread.device(zs(z, -1), y, core),
    ]
    for neighbour in neighbours:
        pl.semaphore_signal(
            barrier, inc=1, device_id=neighbour, device_id_type=pl.DeviceIdType.MESH
        )
    pl.semaphore_wait(barrier, len(neighbours))
    own.wait()
    spread.begin()

    def to_partner(src, dst, i):
        return pltpu.make_async_remote_copy(
            src_ref=src,
            dst_ref=dst,
            send_sem=more_sent.at[i],
            recv_sem=more_arrived.at[i],
            device_id=spread.device(z, y, 1 - core),
            device_id_type=pl.DeviceIdType.MESH,
        )

    exchange = [
        to_partner(q_broad, all_q_broad.at[core], 0),
        to_partner(q_narrow, all_q_narrow.at[core], 1),
    ]
    for copy in exchange:
        copy.start()
    all_q_broad[core] = q_broad[...]
    all_q_narrow[core] = q_narrow[...]
    spread.open_rings()
    for copy in exchange:
        copy.wait_recv()
    prepare(
        core,
        all_q_broad[...].reshape(2 * rows, -1),
        all_q_narrow[...].reshape(2 * rows, -1),
        cosines[...],
        sines[...],
        (key_up_broad, value_up_broad, key_up_narrow, value_up_narrow),
        qt_broad,
        qt_narrow,
        w_key,
        w_value_t,
    )
    spread.landed(*spread.own_chip())
    tools = (qt_broad, qt_narrow, w_key, w_value_t, top, total, acc)

    def block_of(k):
        return held[k // ny, lax.rem(k, ny)].reshape(2 * rows, -1)

    attend_block(block_of(chip), True, *tools)
    for name in spread.order():
        spread.pass_on(name)
    spread.landed(*spread.handed())

    def earlier(k, carried):
        attend_block(block_of(k), False, *tools)
        return carried

    lax.fori_loop(0, chip, earlier, 0)
    broad = jnp.transpose(acc[0:DB] / total[0])
    narrow = jnp.transpose(acc[DB : DB + DN] / total[1])
    finished[...] = (
        jnp.concatenate([broad, narrow], axis=1).astype(bf16).reshape(2, rows, DB + DN)
    )
    result = to_partner(finished.at[1 - core], out.at[core], 2)
    result.start()
    out[core] = finished[core]
    spread.drain()
    for copy in exchange:
        copy.wait_send()
    result.wait()


def attention(geometry, packed, q_broad, q_narrow, cosines, sines, ups):
    nz, ny = geometry[:2]
    rows, width = packed.shape
    vmem = pl.BlockSpec(memory_space=pltpu.VMEM)
    copies = Spread.count(nz, ny)
    return pl.pallas_call(
        functools.partial(attention_kernel, geometry),
        out_shape=jax.ShapeDtypeStruct((2, rows, DB + DN), bf16),
        in_specs=[pl.BlockSpec(memory_space=pl.ANY)] + [vmem] * 8,
        out_specs=vmem,
        scratch_shapes=[
            pltpu.VMEM((nz, ny, 2, rows, width), bf16),
            pltpu.VMEM((2, rows, q_broad.shape[1]), bf16),
            pltpu.VMEM((2, rows, q_narrow.shape[1]), bf16),
            pltpu.VMEM((256, 2 * rows), bf16),
            pltpu.VMEM((128, 2 * rows), bf16),
            pltpu.VMEM((512, 256), bf16),
            pltpu.VMEM((DB + DN, 512), bf16),
            pltpu.VMEM((2, 1, 2 * rows), f32),
            pltpu.VMEM((2, 1, 2 * rows), f32),
            pltpu.VMEM((DB + DN, 2 * rows), f32),
            pltpu.VMEM((2, rows, DB + DN), bf16),
            pltpu.SemaphoreType.DMA,
            pltpu.SemaphoreType.DMA((copies,)),
            pltpu.SemaphoreType.DMA((copies,)),
            pltpu.SemaphoreType.DMA((3,)),
            pltpu.SemaphoreType.DMA((3,)),
        ],
        compiler_params=pltpu.CompilerParams(
            collective_id=0, has_side_effects=True, vmem_limit_bytes=56 * 1024 * 1024
        ),
        cost_estimate=pl.CostEstimate(
            flops=40_000_000_000, bytes_accessed=20_000_000, transcendentals=9_000_000
        ),
        name="attention",
    )(packed, q_broad, q_narrow, cosines, sines, *ups)


def rms_scale(values, norm_gain):
    return (
        values * lax.rsqrt(jnp.mean(values * values, axis=-1, keepdims=True) + norm_eps) * norm_gain
    )


def angles_of(first, count):
    frequency = rope_base ** (-2.0 * jnp.arange(ROPE // 2, dtype=f32) / ROPE)
    positions = (first + jnp.arange(count, dtype=jnp.int32)).astype(f32)
    return positions, frequency


def local(
    resid,
    query_broad,
    query_narrow,
    latent,
    key_rope,
    latent_gain,
    key_up_broad,
    value_up_broad,
    key_up_narrow,
    value_up_narrow,
    out_broad,
    out_narrow,
    post_gain,
    ffn_gain,
    up_weight,
    down_weight,
    ffn_out_gain,
):
    rows = resid.shape[0]
    parts = lax.axis_size("tp")
    share = rows // parts
    me = lax.axis_index("sp")
    ny = NY
    nz = lax.axis_size("sp") // (2 * ny)

    positions, frequency = angles_of(me * rows, rows)
    angles = positions[:, None] * frequency[None, :]
    cosine, sine = jnp.cos(angles), jnp.sin(angles)
    leading, trailing = jnp.split(key_rope.astype(f32), 2, axis=1)
    latent_normed = rms_scale(latent.astype(f32), latent_gain).astype(bf16)
    packed = jnp.concatenate(
        [
            latent_normed,
            jnp.zeros((rows, 64), bf16),
            (leading * cosine - trailing * sine).astype(bf16),
            (trailing * cosine + leading * sine).astype(bf16),
        ],
        axis=1,
    )
    positions, frequency = angles_of((me // 2) * 2 * rows, 2 * rows)
    angles = frequency[:, None] * positions[None, :]
    cosine, sine = jnp.cos(angles), jnp.sin(angles)
    cosines = jnp.concatenate([cosine, cosine], axis=0)
    sines = jnp.concatenate([-sine, sine], axis=0)
    geometry = (nz, ny, 80, 48, 64)
    attn = attention(
        geometry,
        packed,
        query_broad,
        query_narrow,
        cosines,
        sines,
        (key_up_broad, value_up_broad, key_up_narrow, value_up_narrow),
    )
    both = lax.all_gather(
        jnp.concatenate([up_weight, down_weight], axis=1), "sp", axis=0, tiled=True
    )
    up_full, down_full = both[:, : up_weight.shape[1]], both[:, up_weight.shape[1] :]

    pieces = attn.reshape(2, parts, share, DB + DN).transpose(1, 0, 2, 3)
    pieces = lax.all_to_all(pieces, "tp", 0, 0, tiled=True)
    pieces = pieces.reshape(2 * parts, share, DB + DN).transpose(1, 0, 2)
    rows_broad = pieces[:, :, :DB].reshape(share, -1)
    rows_narrow = pieces[:, :, DB:].reshape(share, -1)
    projected = dot(rows_broad, out_broad) + dot(rows_narrow, out_narrow)
    own_resid = lax.dynamic_slice_in_dim(resid, lax.axis_index("tp") * share, share, 0)
    mixed = (own_resid.astype(f32) + rms_scale(projected, post_gain)).astype(bf16)
    normed = rms_scale(mixed.astype(f32), ffn_gain).astype(bf16)
    hidden = jnp.square(
        jax.nn.relu(dot(lax.all_gather(normed, "tp", axis=0, tiled=True), up_full))
    ).astype(bf16)
    ffn = dot(hidden, down_full, LAST).astype(bf16)
    ffn = lax.all_to_all(ffn.reshape(parts, share, -1), "tp", 0, 0, tiled=True)
    ffn = jnp.sum(ffn.astype(f32), axis=0)
    return (mixed.astype(f32) + rms_scale(ffn, ffn_out_gain)).astype(bf16)


def solution(mesh):
    in_specs = (
        P("sp", None),
        P("sp", "tp"),
        P("sp", "tp"),
        P("sp", None),
        P("sp", None),
        P(),
        P(None, "tp"),
        P(None, "tp"),
        P(None, "tp"),
        P(None, "tp"),
        P(),
        P(),
        P(),
        P(),
        P("sp", "tp"),
        P("sp", "tp"),
        P(),
    )
    out_specs = P(("sp", "tp"), None)
    return jax.shard_map(local, mesh=mesh, in_specs=in_specs, out_specs=out_specs, check_vma=False)
```

```python
import functools
import math

import jax
import jax.numpy as jnp
from jax import lax
from jax.experimental import pallas as pl
from jax.experimental.pallas import tpu as pltpu
from jax.sharding import PartitionSpec as P

DB = 128
DN = 64
ROPE = 64
NY = 4

norm_eps = 1e-06
rope_base = 500000.0
broad_unit = (DB + ROPE) ** (-0.5) * math.log2(math.e)
narrow_unit = (DN + ROPE) ** (-0.5) * math.log2(math.e)
f32 = jnp.float32
bf16 = jnp.bfloat16


def dot(a, b, dims=((1,), (0,))):
    return lax.dot_general(a, b, (dims, ((), ())), preferred_element_type=f32)


def picker(shape, pick):
    rows = lax.broadcasted_iota(jnp.int32, shape, 0)
    columns = lax.broadcasted_iota(jnp.int32, shape, 1)
    return jnp.where(pick(rows, columns), 1.0, 0.0).astype(bf16)


LAST = ((1,), (1,))


def prepare(core, q_broad, q_narrow, cosines, sines, refs, qt_broad, qt_narrow, w_key, w_value_t):
    key_up_broad, value_up_broad, key_up_narrow, value_up_narrow = refs
    at = core * (DB + ROPE)
    rows = q_broad.shape[0]
    wide = q_broad.shape[1]
    qt_broad[0:DB] = dot(
        picker((DB, wide), lambda r, k: k == r + at), q_broad, LAST
    ).astype(bf16)
    qt_broad[DB : DB + 64] = jnp.zeros((64, rows), bf16)

    def rotated(value, start):
        straight = dot(picker((64, value.shape[1]), lambda r, k: k == r + start), value, LAST)
        swapped = dot(
            picker(
                (64, value.shape[1]), lambda r, k: k == jnp.where(r < 32, r + 32, r - 32) + start
            ),
            value,
            LAST,
        )
        return (straight * cosines + swapped * sines).astype(bf16)

    qt_broad[DB + 64 : DB + 128] = rotated(q_broad, at + DB)
    at_n = core * (DN + ROPE)
    qt_narrow[0:64] = dot(
        picker((64, q_narrow.shape[1]), lambda r, k: k == r + at_n), q_narrow, LAST
    ).astype(bf16)
    qt_narrow[64:128] = rotated(q_narrow, at_n + DN)
    w_key[:, 0:DB] = key_up_broad[:, pl.ds(pl.multiple_of(core * DB, DB), DB)]
    w_key[:, DB : DB + 128] = dot(
        key_up_narrow[...], picker((128, 128), lambda r, k: (r == k + core * DN) & (k < DN))
    ).astype(bf16)
    w_value_t[0:DB] = dot(
        picker((DB, 2 * DB), lambda r, k: k == r + core * DB), value_up_broad[...], LAST
    ).astype(bf16)
    w_value_t[DB : DB + DN] = dot(
        picker((DN, 2 * DN), lambda r, k: k == r + core * DN), value_up_narrow[...], LAST
    ).astype(bf16)


def attend_block(block, diagonal, qt_broad, qt_narrow, w_key, w_value_t, top, total, acc):
    keys, queries = block.shape[0], qt_broad.shape[1]
    latent = block[:, 0:512]
    expanded = dot(latent, w_key[...])
    key_b = expanded[:, 0:DB].astype(bf16)
    key_n = (expanded[:, DB : DB + 128] + block[:, 512:640].astype(f32)).astype(bf16)
    value_t = dot(w_value_t[...], latent, LAST).astype(bf16)
    score_b = dot(jnp.concatenate([key_b, key_n], axis=1), qt_broad[...])
    score_n = dot(key_n, qt_narrow[...])
    if diagonal:
        allowed = lax.broadcasted_iota(jnp.int32, (keys, queries), 0) <= lax.broadcasted_iota(
            jnp.int32, (keys, queries), 1
        )
    for head, (score, unit, start, size) in enumerate(
        ((score_b, broad_unit, 0, DB), (score_n, narrow_unit, DB, DN))
    ):
        if diagonal:
            score = jnp.where(allowed, score, -1e30)
            peak = jnp.max(score, axis=0, keepdims=True)
        else:
            peak = jnp.maximum(top[head], jnp.max(score, axis=0, keepdims=True))
        weight = jnp.exp2((score - peak) * unit)
        if diagonal:
            weight = jnp.where(allowed, weight, 0.0)
        added = jnp.sum(weight, axis=0, keepdims=True)
        product = dot(value_t[start : start + size], weight.astype(bf16))
        if diagonal:
            total[head] = added
            acc[start : start + size] = product
        else:
            factor = jnp.exp2((top[head] - peak) * unit)
            total[head] = total[head] * factor + added
            acc[start : start + size] = acc[start : start + size] * factor + product
        top[head] = peak


def ring_places(axis_size):
    return lambda at, step: lax.rem(at + step + axis_size, axis_size)


class Spread:
    def __init__(self, held, sent, arrived, place, first, first_cut, rest_cut):
        self.held, self.sent, self.arrived = held, sent, arrived
        self.z, self.y, self.core = place
        self.nz, self.ny, _, self.rows, _ = held.shape
        self.first, self.first_cut, self.rest_cut = first, first_cut, rest_cut
        self.half_z, self.half_y = self.nz // 2, self.ny // 2
        names = [("ay", s, d) for s in (0, 1) for d in (1, -1)]
        for s in range(self.half_z):
            for d in (1, -1):
                names.append(("bz", s, d))
                for ch in (0, 1):
                    if s < self.half_z - 1 or ch == (0 if d == 1 else 1):
                        names.append(("az", s, d, ch))
                        names.append(("pa", s, d, ch))
        for s in (0, 1):
            for d in (1, -1):
                for ch in (0, 1):
                    if s == 0 or ch == (0 if d == 1 else 1):
                        names.append(("by", s, d, ch))
                        names.append(("pb", s, d, ch))
        names += [("pa", -1, 1, 0), ("pa", -1, 1, 1), ("pb", -1, 1, 0)]
        self.index = {name: i for i, name in enumerate(names)}

    @staticmethod
    def count(nz, ny):
        return 4 + (nz // 2) * 2 + 2 * ((nz // 2 - 1) * 4 + 2) + 2 * 6 + 3

    def device(self, z, y, core):
        return {"sp": (z * self.ny + y) * 2 + core}

    def copy(self, name):
        kind, s, d = name[:3]
        zs, ys = ring_places(self.nz), ring_places(self.ny)
        z, y, c, held, first = self.z, self.y, self.core, self.held, self.first
        low, high = pl.ds(0, first), pl.ds(first, self.rows - first)
        i = self.index[name]
        if kind == "ay":
            if s == 1:
                low = (
                    pl.ds(0, self.first_cut)
                    if d == 1
                    else pl.ds(self.first_cut, first - self.first_cut)
                )
            view, to = held.at[z, ys(y, -s * d), c, low], self.device(z, ys(y, d), c)
        elif kind == "bz":
            if s == self.half_z - 1:
                high = (
                    pl.ds(first, self.rest_cut)
                    if d == 1
                    else pl.ds(first + self.rest_cut, self.rows - first - self.rest_cut)
                )
            view, to = held.at[zs(z, -s * d), y, c, high], self.device(zs(z, d), y, c)
        elif kind == "az":
            part = pl.ds(name[3] * self.half_y, self.half_y)
            view, to = held.at[zs(z, -s * d), part, c, low], self.device(zs(z, d), y, c)
        elif kind == "by":
            part = pl.ds(name[3] * self.half_z, self.half_z)
            view, to = held.at[part, ys(y, -s * d), c, high], self.device(z, ys(y, d), c)
        elif kind == "pa":
            part = pl.ds(name[3] * self.half_y, self.half_y)
            view, to = held.at[zs(z, -(s + 1) * d), part, c, low], self.device(z, y, 1 - c)
        else:
            part = pl.ds(0, self.nz) if s == -1 else pl.ds(name[3] * self.half_z, self.half_z)
            view, to = held.at[part, ys(y, -(s + 1) * d), c, high], self.device(z, y, 1 - c)
        return pltpu.make_async_remote_copy(
            src_ref=view,
            dst_ref=view,
            send_sem=self.sent.at[i],
            recv_sem=self.arrived.at[i],
            device_id=to,
            device_id_type=pl.DeviceIdType.MESH,
        )

    def start(self, *names):
        for name in names:
            self.copy(name).start()

    def landed(self, *names):
        for name in names:
            self.copy(name).wait_recv()

    def both(self, kind, s):
        return [n for n in self.index if n[0] == kind and n[1] == s]

    def begin(self):
        self.start(*self.both("ay", 0), *self.both("bz", 0))

    def open_y(self):
        self.landed(*self.both("ay", 0))
        self.start(*self.both("ay", 1))

    def open_z(self):
        self.landed(*self.both("ay", 1))
        self.start(*self.both("az", 0), *self.both("pa", -1))

    def next_z(self, s):
        self.landed(*self.both("bz", s))
        if s + 1 < self.half_z:
            self.start(*self.both("bz", s + 1))
        else:
            self.start(*self.both("by", 0), *self.both("pb", -1))

    def open_rings(self):
        self.open_y()
        self.next_z(0)
        self.open_z()
        for s in range(1, self.half_z):
            self.next_z(s)

    def pass_on(self, name):
        kind, s, d, ch = name
        self.landed(name)
        following = (kind, s + 1, d, ch)
        if following in self.index:
            self.start(following)
        self.start(("p" + kind[0], s, d, ch))

    def order(self):
        names = []
        for s in range(self.half_z):
            if s == self.half_z // 2:
                names += self.both("by", 0)
            if s == self.half_z - 1:
                names += self.both("by", 1)
            names += self.both("az", s)
        return names

    def own_chip(self):
        return [*self.both("pa", -1), *self.both("pb", -1)]

    def handed(self):
        return [n for n in self.index if n[0] in ("pa", "pb") and n[1] >= 0]

    def drain(self):
        for name in self.index:
            self.copy(name).wait_send()


MESH = pl.DeviceIdType.MESH
CHUNK = 512


def layer_kernel(
    geometry,
    rows_hbm,
    q_broad,
    q_narrow,
    cosines,
    sines,
    key_up_broad,
    value_up_broad,
    key_up_narrow,
    value_up_narrow,
    post_gain,
    ffn_gain,
    ffn_out_gain,
    resid_hbm,
    out_broad_hbm,
    out_narrow_hbm,
    up_hbm,
    down_hbm,
    out,
    held,
    weights,
    all_q_broad,
    all_q_narrow,
    qt_broad,
    qt_narrow,
    w_key,
    w_value_t,
    top,
    total,
    acc,
    finished,
    gathered,
    out_broad,
    out_narrow,
    resid,
    wide,
    mixed,
    normed,
    hidden,
    partial,
    partial_sent,
    relayed,
    combined,
    from_far,
    from_near,
    local_sem,
    sent,
    arrived,
    w_sent,
    w_arrived,
    q_sent,
    q_arrived,
    a_sent,
    a_arrived,
    n_sent,
    n_arrived,
    r_sent,
    r_arrived,
):
    nz, ny, parts, cuts, w_cuts = geometry
    me, x = lax.axis_index("sp"), lax.axis_index("tp")
    core = lax.rem(me, 2)
    chip = me // 2
    z, y = chip // ny, lax.rem(chip, ny)
    rows = rows_hbm.shape[0]
    share = rows // parts
    zs, ys, xs = ring_places(nz), ring_places(ny), ring_places(parts)
    spread = Spread(held, sent, arrived, (z, y, core), *cuts)
    w_spread = Spread(weights, w_sent, w_arrived, (z, y, core), *w_cuts)
    model_rows = up_hbm.shape[0]

    own_rows = pltpu.make_async_copy(rows_hbm, held.at[z, y, core], local_sem.at[0])
    own_rows.start()
    loads = [
        (up_hbm, weights.at[z, y, core, pl.ds(0, model_rows)]),
        (down_hbm, weights.at[z, y, core, pl.ds(model_rows, model_rows)]),
        (out_broad_hbm, out_broad),
        (out_narrow_hbm, out_narrow),
        (resid_hbm.at[pl.ds(x * share, share)], resid),
    ]
    loads = [
        pltpu.make_async_copy(src, dst, local_sem.at[i + 1]) for i, (src, dst) in enumerate(loads)
    ]
    for load in loads:
        load.start()

    def tile_peer(offset):
        there = lax.rem(core * parts + x + offset, 2 * parts)
        return there, {
            "sp": (z * ny + y) * 2 + there // parts,
            "tp": lax.rem(there, parts),
        }

    barrier = pltpu.get_barrier_semaphore()
    neighbours = [tile_peer(offset)[1] for offset in range(1, 2 * parts)] + [
        spread.device(z, ys(y, 1), core),
        spread.device(z, ys(y, -1), core),
        spread.device(zs(z, 1), y, core),
        spread.device(zs(z, -1), y, core),
    ]
    for neighbour in neighbours:
        pl.semaphore_signal(barrier, inc=1, device_id=neighbour, device_id_type=MESH)
    pl.semaphore_wait(barrier, len(neighbours))
    own_rows.wait()
    spread.begin()

    def remote(src, dst, sems, i, device):
        return pltpu.make_async_remote_copy(
            src_ref=src,
            dst_ref=dst,
            send_sem=sems[0].at[i],
            recv_sem=sems[1].at[i],
            device_id=device,
            device_id_type=MESH,
        )

    partner = spread.device(z, y, 1 - core)
    q_sems, a_sems, n_sems, r_sems = (
        (q_sent, q_arrived),
        (a_sent, a_arrived),
        (n_sent, n_arrived),
        (r_sent, r_arrived),
    )
    exchange = [
        remote(q_broad, all_q_broad.at[core], q_sems, 0, partner),
        remote(q_narrow, all_q_narrow.at[core], q_sems, 1, partner),
    ]
    for copy in exchange:
        copy.start()
    all_q_broad[core] = q_broad[...]
    all_q_narrow[core] = q_narrow[...]
    spread.open_rings()
    for copy in exchange:
        copy.wait_recv()
    prepare(
        core,
        all_q_broad[...].reshape(2 * rows, -1),
        all_q_narrow[...].reshape(2 * rows, -1),
        cosines[...],
        sines[...],
        (key_up_broad, value_up_broad, key_up_narrow, value_up_narrow),
        qt_broad,
        qt_narrow,
        w_key,
        w_value_t,
    )
    spread.landed(*spread.own_chip())
    tools = (qt_broad, qt_narrow, w_key, w_value_t, top, total, acc)

    def block_of(k):
        return held[k // ny, lax.rem(k, ny)].reshape(2 * rows, -1)

    attend_block(block_of(chip), True, *tools)
    for load in loads:
        load.wait()
    for name in spread.order():
        spread.pass_on(name)
    w_spread.begin()
    spread.landed(*spread.handed())

    def opening():
        w_spread.open_y()
        w_spread.next_z(0)

    def opened():
        w_spread.open_z()
        w_spread.next_z(1)

    turns = {3: opening, 7: opened}
    at = 10
    for s in range(2, w_spread.half_z):
        turns[at] = functools.partial(w_spread.next_z, s)
        at += 3
    w_order = w_spread.order()
    early, late = w_order[:4], w_order[4:]
    for i, name in enumerate(early):
        turns[20 + i] = functools.partial(w_spread.pass_on, name)

    def earlier(k, carried):
        for turn, action in turns.items():
            pl.when(k == turn)(action)

        @pl.when(k < chip)
        def _():
            attend_block(block_of(k), False, *tools)

        return carried

    lax.fori_loop(0, nz * ny, earlier, 0)

    def more_turns(count):
        for _ in range(min(count, len(late))):
            w_spread.pass_on(late.pop(0))

    broad = jnp.transpose(acc[0:DB] / total[0])
    narrow = jnp.transpose(acc[DB : DB + DN] / total[1])
    finished[...] = (
        jnp.concatenate([broad, narrow], axis=1).astype(bf16).reshape(2 * parts, share, DB + DN)
    )
    mine = core * parts + x
    pair = 2 * x + core
    to_owners = []
    for offset in range(1, 2 * parts):
        there, device = tile_peer(offset)
        to_owners.append(remote(finished.at[there], gathered.at[pair], a_sems, offset - 1, device))
    for copy in to_owners:
        copy.start()
    gathered[pair] = finished[mine]
    more_turns(4)
    for copy in to_owners:
        copy.wait_recv()
    rows_broad = jnp.concatenate([gathered[g, :, 0:DB] for g in range(2 * parts)], axis=1)
    rows_narrow = jnp.concatenate([gathered[g, :, DB : DB + DN] for g in range(2 * parts)], axis=1)
    width = out.shape[1]

    def project(n, carried):
        columns = pl.ds(pl.multiple_of(n * CHUNK, CHUNK), CHUNK)
        wide[:, columns] = dot(rows_broad, out_broad[:, columns]) + dot(
            rows_narrow, out_narrow[:, columns]
        )
        return carried

    lax.fori_loop(0, width // CHUNK, project, 0)
    mix = (resid[...].astype(f32) + rms_scale(wide[...], post_gain[...])).astype(bf16)
    mixed[...] = mix
    normed[x] = rms_scale(mix.astype(f32), ffn_gain[...]).astype(bf16)
    right, left = {"tp": xs(x, 1)}, {"tp": xs(x, -1)}
    first_rows, last_rows = pl.ds(0, 32), pl.ds(32, share - 32)
    around = [
        remote(normed.at[x], normed.at[x], n_sems, 0, right),
        remote(normed.at[x], normed.at[x], n_sems, 1, left),
        remote(
            normed.at[xs(x, -1), first_rows], normed.at[xs(x, -1), first_rows], n_sems, 2, right
        ),
        remote(normed.at[xs(x, 1), last_rows], normed.at[xs(x, 1), last_rows], n_sems, 3, left),
    ]
    around[0].start()
    around[1].start()
    more_turns(4)
    around[0].wait_recv()
    around[2].start()
    around[1].wait_recv()
    around[3].start()
    more_turns(len(late))
    around[2].wait_recv()
    around[3].wait_recv()
    w_spread.landed(*w_spread.own_chip(), *w_spread.handed())
    inputs = normed[...].reshape(rows, width)

    def raise_up(n, carried):
        columns = pl.ds(pl.multiple_of(n * CHUNK, CHUNK), CHUNK)
        up = weights[:, :, :, 0:model_rows, columns].reshape(width, CHUNK)
        raised = jnp.maximum(dot(inputs, up), 0.0)
        hidden[:, columns] = (raised * raised).astype(bf16)
        return carried

    lax.fori_loop(0, hidden.shape[1] // CHUNK, raise_up, 0)

    pieces = width // CHUNK
    per_z = 2 * ny * model_rows
    copies = {}
    for n in range(pieces):
        d = 1 if n % 2 == 0 else -1
        columns = slice(n * CHUNK, (n + 1) * CHUNK)
        near, far = {"tp": xs(x, d)}, {"tp": xs(x, -d)}
        copies[n] = (
            remote(partial_sent.at[xs(x, 2), :, columns], relayed.at[n], r_sems, 3 * n, near),
            remote(
                partial_sent.at[xs(x, -d), :, columns],
                from_near.at[:, columns],
                r_sems,
                3 * n + 1,
                far,
            ),
            remote(combined.at[n], from_far.at[:, columns], r_sems, 3 * n + 2, near),
        )

    def lower(n):
        columns = slice(n * CHUNK, (n + 1) * CHUNK)
        zn = CHUNK // per_z
        down = weights[n * zn : (n + 1) * zn, :, :, model_rows : 2 * model_rows].reshape(
            CHUNK, hidden.shape[1]
        )
        sums = dot(hidden[...], down, LAST).reshape(parts, share, CHUNK)
        partial[:, :, columns] = sums
        partial_sent[:, :, columns] = sums.astype(bf16)
        copies[n][0].start()
        copies[n][1].start()

    def relay(n):
        d = 1 if n % 2 == 0 else -1
        columns = slice(n * CHUNK, (n + 1) * CHUNK)
        copies[n][0].wait_recv()
        combined[n] = (partial[xs(x, d), :, columns] + relayed[n].astype(f32)).astype(bf16)
        copies[n][2].start()

    for n in range(pieces):
        lower(n)
        if n > 0:
            relay(n - 1)
    relay(pieces - 1)
    for n in range(pieces):
        copies[n][1].wait_recv()
        copies[n][2].wait_recv()
    ffn = partial[x] + from_near[...].astype(f32) + from_far[...].astype(f32)
    out[...] = (mixed[...].astype(f32) + rms_scale(ffn, ffn_out_gain[...])).astype(bf16)
    spread.drain()
    w_spread.drain()
    for copy in exchange + to_owners + around:
        copy.wait_send()
    for n in range(pieces):
        for copy in copies[n]:
            copy.wait_send()


def rms_scale(values, norm_gain):
    return (
        values * lax.rsqrt(jnp.mean(values * values, axis=-1, keepdims=True) + norm_eps) * norm_gain
    )


def layer(geometry, packed, queries, tables, ups, gains, resid, outs, up_weight, down_weight):
    nz, ny, parts = geometry[:3]
    rows, latent_width = packed.shape
    width = resid.shape[1]
    hidden = up_weight.shape[1]
    share = rows // parts
    model_rows = up_weight.shape[0]
    vmem = pl.BlockSpec(memory_space=pltpu.VMEM)
    anywhere = pl.BlockSpec(memory_space=pl.ANY)
    copies = Spread.count(nz, ny)
    pieces = width // CHUNK
    sems = pltpu.SemaphoreType.DMA
    operands = (packed, *queries, *tables, *ups, *gains, resid, *outs, up_weight, down_weight)
    return pl.pallas_call(
        functools.partial(layer_kernel, geometry),
        out_shape=jax.ShapeDtypeStruct((share, width), bf16),
        in_specs=[anywhere] + [vmem] * 11 + [anywhere] * 5,
        out_specs=vmem,
        scratch_shapes=[
            pltpu.VMEM((nz, ny, 2, rows, latent_width), bf16),
            pltpu.VMEM((nz, ny, 2, 2 * model_rows, hidden), bf16),
            pltpu.VMEM((2, rows, queries[0].shape[1]), bf16),
            pltpu.VMEM((2, rows, queries[1].shape[1]), bf16),
            pltpu.VMEM((256, 2 * rows), bf16),
            pltpu.VMEM((128, 2 * rows), bf16),
            pltpu.VMEM((512, 256), bf16),
            pltpu.VMEM((DB + DN, 512), bf16),
            pltpu.VMEM((2, 1, 2 * rows), f32),
            pltpu.VMEM((2, 1, 2 * rows), f32),
            pltpu.VMEM((DB + DN, 2 * rows), f32),
            pltpu.VMEM((2 * parts, share, DB + DN), bf16),
            pltpu.VMEM((2 * parts, share, DB + DN), bf16),
            pltpu.VMEM(outs[0].shape, bf16),
            pltpu.VMEM(outs[1].shape, bf16),
            pltpu.VMEM((share, width), bf16),
            pltpu.VMEM((share, width), f32),
            pltpu.VMEM((share, width), bf16),
            pltpu.VMEM((parts, share, width), bf16),
            pltpu.VMEM((rows, hidden), bf16),
            pltpu.VMEM((parts, share, width), f32),
            pltpu.VMEM((parts, share, width), bf16),
            pltpu.VMEM((pieces, share, CHUNK), bf16),
            pltpu.VMEM((pieces, share, CHUNK), bf16),
            pltpu.VMEM((share, width), bf16),
            pltpu.VMEM((share, width), bf16),
            sems((6,)),
            sems((copies,)),
            sems((copies,)),
            sems((copies,)),
            sems((copies,)),
            sems((2,)),
            sems((2,)),
            sems((2 * parts - 1,)),
            sems((2 * parts - 1,)),
            sems((4,)),
            sems((4,)),
            sems((3 * pieces,)),
            sems((3 * pieces,)),
        ],
        compiler_params=pltpu.CompilerParams(
            collective_id=0, has_side_effects=True, vmem_limit_bytes=63 * 1024 * 1024
        ),
        cost_estimate=pl.CostEstimate(
            flops=40_000_000_000, bytes_accessed=20_000_000, transcendentals=9_000_000
        ),
        name="layer",
    )(*operands)


def angles_of(first, count):
    frequency = rope_base ** (-2.0 * jnp.arange(ROPE // 2, dtype=f32) / ROPE)
    positions = (first + jnp.arange(count, dtype=jnp.int32)).astype(f32)
    return positions, frequency


def local(
    resid,
    query_broad,
    query_narrow,
    latent,
    key_rope,
    latent_gain,
    key_up_broad,
    value_up_broad,
    key_up_narrow,
    value_up_narrow,
    out_broad,
    out_narrow,
    post_gain,
    ffn_gain,
    up_weight,
    down_weight,
    ffn_out_gain,
):
    rows = resid.shape[0]
    parts = lax.axis_size("tp")
    me = lax.axis_index("sp")
    nz = lax.axis_size("sp") // (2 * NY)

    positions, frequency = angles_of(me * rows, rows)
    angles = positions[:, None] * frequency[None, :]
    cosine, sine = jnp.cos(angles), jnp.sin(angles)
    leading, trailing = jnp.split(key_rope.astype(f32), 2, axis=1)
    latent_normed = rms_scale(latent.astype(f32), latent_gain).astype(bf16)
    packed = jnp.concatenate(
        [
            latent_normed,
            jnp.zeros((rows, 64), bf16),
            (leading * cosine - trailing * sine).astype(bf16),
            (trailing * cosine + leading * sine).astype(bf16),
        ],
        axis=1,
    )
    positions, frequency = angles_of((me // 2) * 2 * rows, 2 * rows)
    angles = frequency[:, None] * positions[None, :]
    cosine, sine = jnp.cos(angles), jnp.sin(angles)
    cosines = jnp.concatenate([cosine, cosine], axis=0)
    sines = jnp.concatenate([-sine, sine], axis=0)
    return layer(
        (nz, NY, parts, (80, 48, 64), (32, 16, 16)),
        packed,
        (query_broad, query_narrow),
        (cosines, sines),
        (key_up_broad, value_up_broad, key_up_narrow, value_up_narrow),
        (post_gain[None, :], ffn_gain[None, :], ffn_out_gain[None, :]),
        resid,
        (out_broad, out_narrow),
        up_weight,
        down_weight,
    )


def solution(mesh):
    in_specs = (
        P("sp", None),
        P("sp", "tp"),
        P("sp", "tp"),
        P("sp", None),
        P("sp", None),
        P(),
        P(None, "tp"),
        P(None, "tp"),
        P(None, "tp"),
        P(None, "tp"),
        P(),
        P(),
        P(),
        P(),
        P("sp", "tp"),
        P("sp", "tp"),
        P(),
    )
    out_specs = P(("sp", "tp"), None)
    return jax.shard_map(local, mesh=mesh, in_specs=in_specs, out_specs=out_specs, check_vma=False)
```

```python
import functools
import math

import jax
import jax.numpy as jnp
from jax import lax
from jax.experimental import pallas as pl
from jax.experimental.pallas import tpu as pltpu
from jax.sharding import PartitionSpec as P

DB = 128
DN = 64
ROPE = 64
NY = 4

norm_eps = 1e-06
rope_base = 500000.0
broad_unit = (DB + ROPE) ** (-0.5) * math.log2(math.e)
narrow_unit = (DN + ROPE) ** (-0.5) * math.log2(math.e)
f32 = jnp.float32
bf16 = jnp.bfloat16


def dot(a, b, dims=((1,), (0,))):
    return lax.dot_general(a, b, (dims, ((), ())), preferred_element_type=f32)


def picker(shape, pick):
    rows = lax.broadcasted_iota(jnp.int32, shape, 0)
    columns = lax.broadcasted_iota(jnp.int32, shape, 1)
    return jnp.where(pick(rows, columns), 1.0, 0.0).astype(bf16)


LAST = ((1,), (1,))


def prepare(core, q_broad, q_narrow, cosines, sines, refs, qt_broad, qt_narrow, w_key, w_value_t):
    key_up_broad, value_up_broad, key_up_narrow, value_up_narrow = refs
    at = core * (DB + ROPE)
    rows = q_broad.shape[0]
    wide = q_broad.shape[1]
    qt_broad[0:DB] = dot(
        picker((DB, wide), lambda r, k: k == r + at), q_broad, LAST
    ).astype(bf16)
    qt_broad[DB : DB + 64] = jnp.zeros((64, rows), bf16)

    def rotated(value, start):
        straight = dot(picker((64, value.shape[1]), lambda r, k: k == r + start), value, LAST)
        swapped = dot(
            picker(
                (64, value.shape[1]), lambda r, k: k == jnp.where(r < 32, r + 32, r - 32) + start
            ),
            value,
            LAST,
        )
        return (straight * cosines + swapped * sines).astype(bf16)

    qt_broad[DB + 64 : DB + 128] = rotated(q_broad, at + DB)
    at_n = core * (DN + ROPE)
    qt_narrow[0:64] = dot(
        picker((64, q_narrow.shape[1]), lambda r, k: k == r + at_n), q_narrow, LAST
    ).astype(bf16)
    qt_narrow[64:128] = rotated(q_narrow, at_n + DN)
    w_key[:, 0:DB] = key_up_broad[:, pl.ds(pl.multiple_of(core * DB, DB), DB)]
    w_key[:, DB : DB + 128] = dot(
        key_up_narrow[...], picker((128, 128), lambda r, k: (r == k + core * DN) & (k < DN))
    ).astype(bf16)
    w_value_t[0:DB] = dot(
        picker((DB, 2 * DB), lambda r, k: k == r + core * DB), value_up_broad[...], LAST
    ).astype(bf16)
    w_value_t[DB : DB + DN] = dot(
        picker((DN, 2 * DN), lambda r, k: k == r + core * DN), value_up_narrow[...], LAST
    ).astype(bf16)


def attend_block(block, diagonal, qt_broad, qt_narrow, w_key, w_value_t, top, total, acc):
    keys, queries = block.shape[0], qt_broad.shape[1]
    latent = block[:, 0:512]
    expanded = dot(latent, w_key[...])
    key_b = expanded[:, 0:DB].astype(bf16)
    key_n = (expanded[:, DB : DB + 128] + block[:, 512:640].astype(f32)).astype(bf16)
    value_t = dot(w_value_t[...], latent, LAST).astype(bf16)
    score_b = dot(jnp.concatenate([key_b, key_n], axis=1), qt_broad[...])
    score_n = dot(key_n, qt_narrow[...])
    if diagonal:
        allowed = lax.broadcasted_iota(jnp.int32, (keys, queries), 0) <= lax.broadcasted_iota(
            jnp.int32, (keys, queries), 1
        )
    for head, (score, unit, start, size) in enumerate(
        ((score_b, broad_unit, 0, DB), (score_n, narrow_unit, DB, DN))
    ):
        if diagonal:
            score = jnp.where(allowed, score, -1e30)
            peak = jnp.max(score, axis=0, keepdims=True)
        else:
            peak = jnp.maximum(top[head], jnp.max(score, axis=0, keepdims=True))
        weight = jnp.exp2((score - peak) * unit)
        if diagonal:
            weight = jnp.where(allowed, weight, 0.0)
        added = jnp.sum(weight, axis=0, keepdims=True)
        product = dot(value_t[start : start + size], weight.astype(bf16))
        if diagonal:
            total[head] = added
            acc[start : start + size] = product
        else:
            factor = jnp.exp2((top[head] - peak) * unit)
            total[head] = total[head] * factor + added
            acc[start : start + size] = acc[start : start + size] * factor + product
        top[head] = peak


def ring_places(axis_size):
    return lambda at, step: lax.rem(at + step + axis_size, axis_size)


def offset_of(k):
    return (k + 1) // 2 * (1 if k % 2 else -1)


Y_BLOCKS = (0, -1, 1, 2)


def copies_of(nz, ny, crossed):
    assert ny == 4 and nz % 4 == 0
    last = nz // 2 - 1
    tasks = {}
    for d in (1, -1):
        tasks["ay", 0, d] = (("y", d), "a", 1, ())
        tasks["ay", 1, d] = (("y", d), "a" + "+-"[d < 0], 1, (("ay", 0, d),))
    source = {0: (), -1: (("ay", 0, 1),), 1: (("ay", 0, -1),), 2: (("ay", 1, 1), ("ay", 1, -1))}
    for s in range(last + 1):
        for j, at in enumerate(Y_BLOCKS):
            for d in (1, -1):
                if s < last or d == (1 if j % 2 == 0 else -1):
                    before = source[at] if s == 0 else (("az", s - 1, d, j),)
                    tasks["az", s, d, j] = (("z", d), "a", 1, before)
        for d in (1, -1):
            rows = "b" if s < last else "b" + "+-"[d < 0]
            tasks["bz", s, d] = (("z", d), rows, 1, () if s == 0 else (("bz", s - 1, d),))
    planes = {}
    for k in range(nz):
        off = offset_of(k)
        came = -1 if off > 0 else 1
        if k == 0:
            column, plane = (), tuple(tasks_ for tasks_ in tasks if tasks_[0] == "ay")
        elif k == nz - 1:
            column = (("bz", last, 1), ("bz", last, -1))
            plane = tuple(("az", last, 1 if j % 2 == 0 else -1, j) for j in range(ny)) + column
        else:
            column = (("bz", abs(off) - 1, came),)
            plane = tuple(("az", abs(off) - 1, came, j) for j in range(ny)) + column
        far = 1 if k % 2 == 0 else -1
        for d in (1, -1):
            tasks["by", k, 0, d] = (("y", d), "b", 1, column)
        tasks["by", k, 1, far] = (("y", far), "b", 1, (("by", k, 0, far),))
        plane += (("by", k, 0, 1), ("by", k, 0, -1), ("by", k, 1, far))
        tasks["hand", k] = (("c", 0), "ab", ny, plane)
        if crossed:
            for d in (1, -1):
                tasks["x", k, d] = (("x", d), "ab", ny // 2, plane)
            tasks["handx", k] = (("c", 0), "ab", ny, (("x", k, 1), ("x", k, -1)))
            plane += (("x", k, 1), ("x", k, -1), ("handx", k))
        planes[k] = plane + (("hand", k),)
    return tasks, planes


def foreseen(groups, delays, link_rate=46.0, chip_rate=450.0, latency=2.0):
    landed, waiting, free, now = {}, set(), {}, 0.0
    pending = []
    for g, (tasks, sizes) in groups.items():
        for name in tasks:
            waiting.add((g, name))
    started = set()

    def start_ready(time):
        for g, (tasks, sizes) in groups.items():
            if time < delays[g]:
                continue
            for name, (link, rows, blocks, before) in tasks.items():
                key = (g, name)
                if key in started or any((g, b) not in landed for b in before):
                    continue
                started.add(key)
                rate = chip_rate if link[0] == "c" else link_rate
                begin = max(time, free.get(link, 0.0))
                end = begin + sizes[rows] * blocks / rate / 1e3
                free[link] = end
                pending.append((end + (1.0 if link[0] == "c" else latency), key))

    times = sorted(set(delays.values()))
    while True:
        for t in times:
            if t <= now:
                start_ready(now)
        later = [t for t in times if t > now]
        upcoming = min(pending)[0] if pending else None
        if upcoming is None and not later:
            break
        if upcoming is None or (later and later[0] < upcoming):
            now = later[0]
            continue
        pending.sort()
        now, key = pending.pop(0)
        landed[key] = now
    return landed


class Web:
    def __init__(self, held, sems, place, tasks, cuts, crossed):
        self.held, self.sent, self.arrived = held, *sems
        self.z, self.y, self.core, self.x, self.parts = place
        self.nz, self.ny = held.shape[:2]
        self.tasks = tasks
        self.index = {name: i for i, name in enumerate(tasks)}
        a, b, a_cut, b_cut = cuts
        self.spans = {
            "a": (0, a),
            "b": (a, b),
            "a+": (0, a_cut),
            "a-": (a_cut, a - a_cut),
            "b+": (a, b_cut),
            "b-": (a + b_cut, b - b_cut),
            "ab": (0, a + b),
        }
        parity = lax.rem(self.x, 2) if crossed else 0
        self.base = parity * (a + b)
        self.other_base = (1 - parity) * (a + b)

    def sizes(self):
        row = self.held.shape[4] * 2
        return {key: size * row for key, (_, size) in self.spans.items()}

    def rows(self, key, base):
        start, size = self.spans[key]
        if isinstance(base, int):
            return pl.ds(base + start, size)
        return pl.ds(pl.multiple_of(base + start, 16), size)

    def device(self, z, y, core):
        return {"sp": (z * self.ny + y) * 2 + core}

    def copy(self, name):
        kind = name[0]
        link, key, _, _ = self.tasks[name]
        zs, ys, xs = ring_places(self.nz), ring_places(self.ny), ring_places(self.parts)
        z, y, c = self.z, self.y, self.core
        rows = self.rows(key, self.other_base if kind == "handx" else self.base)
        if kind == "ay":
            at = (z, ys(y, -name[1] * name[2]))
        elif kind == "az":
            at = (zs(z, -name[1] * name[2]), ys(y, Y_BLOCKS[name[3]]))
        elif kind == "bz":
            at = (zs(z, -name[1] * name[2]), y)
        elif kind == "by":
            at = (zs(z, offset_of(name[1])), ys(y, -name[2] * name[3]))
        elif kind == "x":
            half = self.ny // 2
            at = (zs(z, offset_of(name[1])), pl.ds(0 if name[2] == 1 else half, half))
        else:
            at = (zs(z, offset_of(name[1])), pl.ds(0, self.ny))
        view = self.held.at[at[0], at[1], c, rows]
        axis, d = link
        to = {
            "y": lambda: self.device(z, ys(y, d), c),
            "z": lambda: self.device(zs(z, d), y, c),
            "c": lambda: self.device(z, y, 1 - c),
            "x": lambda: {"tp": xs(self.x, d)},
        }[axis]()
        i = self.index[name]
        return pltpu.make_async_remote_copy(
            src_ref=view,
            dst_ref=view,
            send_sem=self.sent.at[i],
            recv_sem=self.arrived.at[i],
            device_id=to,
            device_id_type=pl.DeviceIdType.MESH,
        )

    def drain(self):
        for name in self.tasks:
            self.copy(name).wait_send()


def program_of(webs, delays):
    times = foreseen({g: (web.tasks, web.sizes()) for g, web in webs.items()}, delays)
    seen, begun, lines = set(), set(), []

    def ready(group):
        names = [
            name
            for name, (_, _, _, before) in webs[group].tasks.items()
            if (group, name) not in begun and all((group, b) in seen for b in before)
        ]
        begun.update((group, name) for name in names)
        return [(group, name) for name in names]

    stops = [(delay, 0, group, None) for group, delay in delays.items()]
    stops += [(time, 1, group, name) for (group, name), time in times.items()]
    for time, _, group, name in sorted(stops, key=lambda s: (s[0], s[1], str(s[2:]))):
        if name is not None:
            seen.add((group, name))
        lines.append((time, None if name is None else (group, name), ready(group)))
    return lines, times


MESH = pl.DeviceIdType.MESH
CHUNK = 512
W_DELAY = 18.0
BLOCK_US = 1.0


def layer_kernel(
    geometry,
    rows_hbm,
    q_broad,
    q_narrow,
    cosines,
    sines,
    key_up_broad,
    value_up_broad,
    key_up_narrow,
    value_up_narrow,
    post_gain,
    ffn_gain,
    ffn_out_gain,
    resid_hbm,
    out_broad_hbm,
    out_narrow_hbm,
    up_hbm,
    down_hbm,
    out,
    held,
    weights,
    all_q_broad,
    all_q_narrow,
    qt_broad,
    qt_narrow,
    w_key,
    w_value_t,
    top,
    total,
    acc,
    finished,
    gathered,
    out_broad,
    out_narrow,
    resid,
    wide,
    mixed,
    normed,
    hidden,
    partial,
    partial_sent,
    relayed,
    combined,
    from_far,
    from_near,
    local_sem,
    sent,
    arrived,
    w_sent,
    w_arrived,
    q_sent,
    q_arrived,
    a_sent,
    a_arrived,
    n_sent,
    n_arrived,
    r_sent,
    r_arrived,
):
    nz, ny, parts, cuts, w_cuts = geometry
    me, x = lax.axis_index("sp"), lax.axis_index("tp")
    core = lax.rem(me, 2)
    chip = me // 2
    z, y = chip // ny, lax.rem(chip, ny)
    rows = rows_hbm.shape[0]
    share = rows // parts
    zs, ys, xs = ring_places(nz), ring_places(ny), ring_places(parts)
    place = (z, y, core, x, parts)
    tasks, planes = copies_of(nz, ny, True)
    w_tasks, w_planes = copies_of(nz, ny, False)
    spread = Web(held, (sent, arrived), place, tasks, cuts, True)
    w_spread = Web(weights, (w_sent, w_arrived), place, w_tasks, w_cuts, False)
    webs = {"l": spread, "w": w_spread}
    lines, times = program_of(webs, {"l": 0.0, "w": W_DELAY})
    model_rows = up_hbm.shape[0]

    own_part = spread.rows("ab", spread.base)
    own_rows = pltpu.make_async_copy(
        rows_hbm.at[own_part], held.at[z, y, core, own_part], local_sem.at[0]
    )
    own_rows.start()
    loads = [
        (up_hbm, weights.at[z, y, core, pl.ds(0, model_rows)]),
        (down_hbm, weights.at[z, y, core, pl.ds(model_rows, model_rows)]),
        (out_broad_hbm, out_broad),
        (out_narrow_hbm, out_narrow),
        (resid_hbm.at[pl.ds(x * share, share)], resid),
    ]
    loads = [
        pltpu.make_async_copy(src, dst, local_sem.at[i + 1]) for i, (src, dst) in enumerate(loads)
    ]
    for load in loads:
        load.start()

    def tile_peer(offset):
        there = lax.rem(core * parts + x + offset, 2 * parts)
        return there, {
            "sp": (z * ny + y) * 2 + there // parts,
            "tp": lax.rem(there, parts),
        }

    barrier = pltpu.get_barrier_semaphore()
    neighbours = [tile_peer(offset)[1] for offset in range(1, 2 * parts)] + [
        spread.device(z, ys(y, 1), core),
        spread.device(z, ys(y, -1), core),
        spread.device(zs(z, 1), y, core),
        spread.device(zs(z, -1), y, core),
    ]
    for neighbour in neighbours:
        pl.semaphore_signal(barrier, inc=1, device_id=neighbour, device_id_type=MESH)
    pl.semaphore_wait(barrier, len(neighbours))
    own_rows.wait()

    def carry_out(line):
        _, landing, starts = line
        if landing is not None:
            webs[landing[0]].copy(landing[1]).wait_recv()
        for group, name in starts:
            webs[group].copy(name).start()

    carry_out(lines.pop(0))

    def remote(src, dst, sems, i, device):
        return pltpu.make_async_remote_copy(
            src_ref=src,
            dst_ref=dst,
            send_sem=sems[0].at[i],
            recv_sem=sems[1].at[i],
            device_id=device,
            device_id_type=MESH,
        )

    partner = spread.device(z, y, 1 - core)
    q_sems, a_sems, n_sems, r_sems = (
        (q_sent, q_arrived),
        (a_sent, a_arrived),
        (n_sent, n_arrived),
        (r_sent, r_arrived),
    )
    exchange = [
        remote(q_broad, all_q_broad.at[core], q_sems, 0, partner),
        remote(q_narrow, all_q_narrow.at[core], q_sems, 1, partner),
    ]
    for copy in exchange:
        copy.start()
    all_q_broad[core] = q_broad[...]
    all_q_narrow[core] = q_narrow[...]
    for copy in exchange:
        copy.wait_recv()
    prepare(
        core,
        all_q_broad[...].reshape(2 * rows, -1),
        all_q_narrow[...].reshape(2 * rows, -1),
        cosines[...],
        sines[...],
        (key_up_broad, value_up_broad, key_up_narrow, value_up_narrow),
        qt_broad,
        qt_narrow,
        w_key,
        w_value_t,
    )
    for load in loads:
        load.wait()
    ready = [max(times["l", name] for name in planes[k]) for k in range(nz)]

    def carry_out_until(time):
        while lines and lines[0][0] <= time:
            carry_out(lines.pop(0))

    carry_out_until(ready[0])
    tools = (qt_broad, qt_narrow, w_key, w_value_t, top, total, acc)

    def block_of(at_z, at_y):
        return held[at_z, at_y].reshape(2 * rows, -1)

    attend_block(block_of(z, y), True, *tools)

    turns, clock = {}, ready[0] + 1.2
    for step in range(nz * ny):
        clock = max(clock, ready[step // ny])
        while lines and lines[0][0] <= clock:
            turns.setdefault(step, []).append(lines.pop(0))
        clock += BLOCK_US

    def earlier(step, carried):
        for turn, due in turns.items():

            @pl.when(step == turn)
            def _(due=due):
                for line in due:
                    carry_out(line)

        k = step // ny
        half = (k + 1) // 2
        at_z = zs(z, half * (2 * lax.rem(k, 2) - 1))
        at_y = lax.rem(step, ny)

        @pl.when(at_z * ny + at_y < chip)
        def _():
            attend_block(block_of(at_z, at_y), False, *tools)

        return carried

    lax.fori_loop(0, nz * ny, earlier, 0)

    broad = jnp.transpose(acc[0:DB] / total[0])
    narrow = jnp.transpose(acc[DB : DB + DN] / total[1])
    finished[...] = (
        jnp.concatenate([broad, narrow], axis=1).astype(bf16).reshape(2 * parts, share, DB + DN)
    )
    mine = core * parts + x
    pair = 2 * x + core
    to_owners = []
    for offset in range(1, 2 * parts):
        there, device = tile_peer(offset)
        to_owners.append(remote(finished.at[there], gathered.at[pair], a_sems, offset - 1, device))
    for copy in to_owners:
        copy.start()
    gathered[pair] = finished[mine]
    carry_out_until(clock + 2.0)
    for copy in to_owners:
        copy.wait_recv()
    rows_broad = jnp.concatenate([gathered[g, :, 0:DB] for g in range(2 * parts)], axis=1)
    rows_narrow = jnp.concatenate([gathered[g, :, DB : DB + DN] for g in range(2 * parts)], axis=1)
    width = out.shape[1]

    def project(n, carried):
        columns = pl.ds(pl.multiple_of(n * CHUNK, CHUNK), CHUNK)
        wide[:, columns] = dot(rows_broad, out_broad[:, columns]) + dot(
            rows_narrow, out_narrow[:, columns]
        )
        return carried

    lax.fori_loop(0, width // CHUNK, project, 0)
    mix = (resid[...].astype(f32) + rms_scale(wide[...], post_gain[...])).astype(bf16)
    mixed[...] = mix
    normed[x] = rms_scale(mix.astype(f32), ffn_gain[...]).astype(bf16)
    right, left = {"tp": xs(x, 1)}, {"tp": xs(x, -1)}
    first_rows, last_rows = pl.ds(0, 32), pl.ds(32, share - 32)
    around = [
        remote(normed.at[x], normed.at[x], n_sems, 0, right),
        remote(normed.at[x], normed.at[x], n_sems, 1, left),
        remote(
            normed.at[xs(x, -1), first_rows], normed.at[xs(x, -1), first_rows], n_sems, 2, right
        ),
        remote(normed.at[xs(x, 1), last_rows], normed.at[xs(x, 1), last_rows], n_sems, 3, left),
    ]
    around[0].start()
    around[1].start()
    carry_out_until(clock + 10.0)
    around[0].wait_recv()
    around[2].start()
    around[1].wait_recv()
    around[3].start()
    while lines:
        carry_out(lines.pop(0))
    around[2].wait_recv()
    around[3].wait_recv()
    inputs = normed[...].reshape(rows, width)

    def raise_up(n, carried):
        columns = pl.ds(pl.multiple_of(n * CHUNK, CHUNK), CHUNK)
        up = weights[:, :, :, 0:model_rows, columns].reshape(width, CHUNK)
        raised = jnp.maximum(dot(inputs, up), 0.0)
        hidden[:, columns] = (raised * raised).astype(bf16)
        return carried

    lax.fori_loop(0, hidden.shape[1] // CHUNK, raise_up, 0)

    pieces = width // CHUNK
    per_z = 2 * ny * model_rows
    copies = {}
    for n in range(pieces):
        d = 1 if n % 2 == 0 else -1
        columns = slice(n * CHUNK, (n + 1) * CHUNK)
        near, far = {"tp": xs(x, d)}, {"tp": xs(x, -d)}
        copies[n] = (
            remote(partial_sent.at[xs(x, 2), :, columns], relayed.at[n], r_sems, 3 * n, near),
            remote(
                partial_sent.at[xs(x, -d), :, columns],
                from_near.at[:, columns],
                r_sems,
                3 * n + 1,
                far,
            ),
            remote(combined.at[n], from_far.at[:, columns], r_sems, 3 * n + 2, near),
        )

    def lower(n):
        columns = slice(n * CHUNK, (n + 1) * CHUNK)
        zn = CHUNK // per_z
        down = weights[n * zn : (n + 1) * zn, :, :, model_rows : 2 * model_rows].reshape(
            CHUNK, hidden.shape[1]
        )
        sums = dot(hidden[...], down, LAST).reshape(parts, share, CHUNK)
        partial[:, :, columns] = sums
        partial_sent[:, :, columns] = sums.astype(bf16)
        copies[n][0].start()
        copies[n][1].start()

    def relay(n):
        d = 1 if n % 2 == 0 else -1
        columns = slice(n * CHUNK, (n + 1) * CHUNK)
        copies[n][0].wait_recv()
        combined[n] = (partial[xs(x, d), :, columns] + relayed[n].astype(f32)).astype(bf16)
        copies[n][2].start()

    for n in range(pieces):
        lower(n)
        if n > 0:
            relay(n - 1)
    relay(pieces - 1)
    for n in range(pieces):
        copies[n][1].wait_recv()
        copies[n][2].wait_recv()
    ffn = partial[x] + from_near[...].astype(f32) + from_far[...].astype(f32)
    out[...] = (mixed[...].astype(f32) + rms_scale(ffn, ffn_out_gain[...])).astype(bf16)
    spread.drain()
    w_spread.drain()
    for copy in exchange + to_owners + around:
        copy.wait_send()
    for n in range(pieces):
        for copy in copies[n]:
            copy.wait_send()


def rms_scale(values, norm_gain):
    return (
        values * lax.rsqrt(jnp.mean(values * values, axis=-1, keepdims=True) + norm_eps) * norm_gain
    )


def layer(geometry, packed, queries, tables, ups, gains, resid, outs, up_weight, down_weight):
    nz, ny, parts = geometry[:3]
    rows, latent_width = packed.shape
    width = resid.shape[1]
    hidden = up_weight.shape[1]
    share = rows // parts
    model_rows = up_weight.shape[0]
    vmem = pl.BlockSpec(memory_space=pltpu.VMEM)
    anywhere = pl.BlockSpec(memory_space=pl.ANY)
    copies = len(copies_of(nz, ny, True)[0])
    w_copies = len(copies_of(nz, ny, False)[0])
    pieces = width // CHUNK
    sems = pltpu.SemaphoreType.DMA
    operands = (packed, *queries, *tables, *ups, *gains, resid, *outs, up_weight, down_weight)
    return pl.pallas_call(
        functools.partial(layer_kernel, geometry),
        out_shape=jax.ShapeDtypeStruct((share, width), bf16),
        in_specs=[anywhere] + [vmem] * 11 + [anywhere] * 5,
        out_specs=vmem,
        scratch_shapes=[
            pltpu.VMEM((nz, ny, 2, rows, latent_width), bf16),
            pltpu.VMEM((nz, ny, 2, 2 * model_rows, hidden), bf16),
            pltpu.VMEM((2, rows, queries[0].shape[1]), bf16),
            pltpu.VMEM((2, rows, queries[1].shape[1]), bf16),
            pltpu.VMEM((256, 2 * rows), bf16),
            pltpu.VMEM((128, 2 * rows), bf16),
            pltpu.VMEM((512, 256), bf16),
            pltpu.VMEM((DB + DN, 512), bf16),
            pltpu.VMEM((2, 1, 2 * rows), f32),
            pltpu.VMEM((2, 1, 2 * rows), f32),
            pltpu.VMEM((DB + DN, 2 * rows), f32),
            pltpu.VMEM((2 * parts, share, DB + DN), bf16),
            pltpu.VMEM((2 * parts, share, DB + DN), bf16),
            pltpu.VMEM(outs[0].shape, bf16),
            pltpu.VMEM(outs[1].shape, bf16),
            pltpu.VMEM((share, width), bf16),
            pltpu.VMEM((share, width), f32),
            pltpu.VMEM((share, width), bf16),
            pltpu.VMEM((parts, share, width), bf16),
            pltpu.VMEM((rows, hidden), bf16),
            pltpu.VMEM((parts, share, width), f32),
            pltpu.VMEM((parts, share, width), bf16),
            pltpu.VMEM((pieces, share, CHUNK), bf16),
            pltpu.VMEM((pieces, share, CHUNK), bf16),
            pltpu.VMEM((share, width), bf16),
            pltpu.VMEM((share, width), bf16),
            sems((6,)),
            sems((copies,)),
            sems((copies,)),
            sems((w_copies,)),
            sems((w_copies,)),
            sems((2,)),
            sems((2,)),
            sems((2 * parts - 1,)),
            sems((2 * parts - 1,)),
            sems((4,)),
            sems((4,)),
            sems((3 * pieces,)),
            sems((3 * pieces,)),
        ],
        compiler_params=pltpu.CompilerParams(
            collective_id=0, has_side_effects=True, vmem_limit_bytes=63 * 1024 * 1024
        ),
        cost_estimate=pl.CostEstimate(
            flops=40_000_000_000, bytes_accessed=20_000_000, transcendentals=9_000_000
        ),
        name="layer",
    )(*operands)


def angles_of(first, count):
    frequency = rope_base ** (-2.0 * jnp.arange(ROPE // 2, dtype=f32) / ROPE)
    positions = (first + jnp.arange(count, dtype=jnp.int32)).astype(f32)
    return positions, frequency


def local(
    resid,
    query_broad,
    query_narrow,
    latent,
    key_rope,
    latent_gain,
    key_up_broad,
    value_up_broad,
    key_up_narrow,
    value_up_narrow,
    out_broad,
    out_narrow,
    post_gain,
    ffn_gain,
    up_weight,
    down_weight,
    ffn_out_gain,
):
    rows = resid.shape[0]
    parts = lax.axis_size("tp")
    me = lax.axis_index("sp")
    nz = lax.axis_size("sp") // (2 * NY)

    positions, frequency = angles_of(me * rows, rows)
    angles = positions[:, None] * frequency[None, :]
    cosine, sine = jnp.cos(angles), jnp.sin(angles)
    leading, trailing = jnp.split(key_rope.astype(f32), 2, axis=1)
    latent_normed = rms_scale(latent.astype(f32), latent_gain).astype(bf16)
    packed = jnp.concatenate(
        [
            latent_normed,
            jnp.zeros((rows, 64), bf16),
            (leading * cosine - trailing * sine).astype(bf16),
            (trailing * cosine + leading * sine).astype(bf16),
        ],
        axis=1,
    )
    positions, frequency = angles_of((me // 2) * 2 * rows, 2 * rows)
    angles = frequency[:, None] * positions[None, :]
    cosine, sine = jnp.cos(angles), jnp.sin(angles)
    cosines = jnp.concatenate([cosine, cosine], axis=0)
    sines = jnp.concatenate([-sine, sine], axis=0)
    return layer(
        (nz, NY, parts, (32, 64, 16, 32), (32, 32, 16, 16)),
        packed,
        (query_broad, query_narrow),
        (cosines, sines),
        (key_up_broad, value_up_broad, key_up_narrow, value_up_narrow),
        (post_gain[None, :], ffn_gain[None, :], ffn_out_gain[None, :]),
        resid,
        (out_broad, out_narrow),
        up_weight,
        down_weight,
    )


def solution(mesh):
    in_specs = (
        P("sp", None),
        P("sp", "tp"),
        P("sp", "tp"),
        P("sp", None),
        P("sp", None),
        P(),
        P(None, "tp"),
        P(None, "tp"),
        P(None, "tp"),
        P(None, "tp"),
        P(),
        P(),
        P(),
        P(),
        P("sp", "tp"),
        P("sp", "tp"),
        P(),
    )
    out_specs = P(("sp", "tp"), None)
    return jax.shard_map(local, mesh=mesh, in_specs=in_specs, out_specs=out_specs, check_vma=False)
```

```python
import functools
import math

import jax
import jax.numpy as jnp
from jax import lax
from jax.experimental import pallas as pl
from jax.experimental.pallas import tpu as pltpu
from jax.sharding import PartitionSpec as P

DB = 128
DN = 64
ROPE = 64
NY = 4

norm_eps = 1e-06
rope_base = 500000.0
broad_unit = (DB + ROPE) ** (-0.5) * math.log2(math.e)
narrow_unit = (DN + ROPE) ** (-0.5) * math.log2(math.e)
f32 = jnp.float32
bf16 = jnp.bfloat16


def dot(a, b, dims=((1,), (0,))):
    return lax.dot_general(a, b, (dims, ((), ())), preferred_element_type=f32)


def picker(shape, pick):
    rows = lax.broadcasted_iota(jnp.int32, shape, 0)
    columns = lax.broadcasted_iota(jnp.int32, shape, 1)
    return jnp.where(pick(rows, columns), 1.0, 0.0).astype(bf16)


LAST = ((1,), (1,))
FIRST = ((0,), (0,))


def prepare(core, q_broad, q_narrow, cosines, sines, refs, qt_broad, qt_narrow, w_key, w_value_t):
    key_up_broad, value_up_broad, key_up_narrow, value_up_narrow = refs
    at = core * (DB + ROPE)
    rows = q_broad.shape[0]
    wide = q_broad.shape[1]
    qt_broad[0:DB] = dot(
        picker((DB, wide), lambda r, k: k == r + at), q_broad, LAST
    ).astype(bf16)
    qt_broad[DB : DB + 64] = jnp.zeros((64, rows), bf16)

    def rotated(value, start):
        straight = dot(picker((64, value.shape[1]), lambda r, k: k == r + start), value, LAST)
        swapped = dot(
            picker(
                (64, value.shape[1]), lambda r, k: k == jnp.where(r < 32, r + 32, r - 32) + start
            ),
            value,
            LAST,
        )
        return (straight * cosines + swapped * sines).astype(bf16)

    qt_broad[DB + 64 : DB + 128] = rotated(q_broad, at + DB)
    at_n = core * (DN + ROPE)
    qt_narrow[0:64] = dot(
        picker((64, q_narrow.shape[1]), lambda r, k: k == r + at_n), q_narrow, LAST
    ).astype(bf16)
    qt_narrow[64:128] = rotated(q_narrow, at_n + DN)
    w_key[:, 0:DB] = key_up_broad[:, pl.ds(pl.multiple_of(core * DB, DB), DB)]
    w_key[:, DB : DB + 128] = dot(
        key_up_narrow[...], picker((128, 128), lambda r, k: (r == k + core * DN) & (k < DN))
    ).astype(bf16)
    w_value_t[0:DB] = dot(
        picker((DB, 2 * DB), lambda r, k: k == r + core * DB), value_up_broad[...], LAST
    ).astype(bf16)
    w_value_t[DB : DB + DN] = dot(
        picker((DN, 2 * DN), lambda r, k: k == r + core * DN), value_up_narrow[...], LAST
    ).astype(bf16)


def attend_block(block, diagonal, qt_broad, qt_narrow, w_key, w_value_t, top, total, acc):
    keys, queries = block.shape[0], qt_broad.shape[1]
    latent = block[:, 0:512]
    expanded = dot(latent, w_key[...])
    key_b = expanded[:, 0:DB].astype(bf16)
    key_n = (expanded[:, DB : DB + 128] + block[:, 512:640].astype(f32)).astype(bf16)
    value_t = dot(w_value_t[...], latent, LAST).astype(bf16)
    score_b = dot(jnp.concatenate([key_b, key_n], axis=1), qt_broad[...])
    score_n = dot(key_n, qt_narrow[...])
    if diagonal:
        allowed = lax.broadcasted_iota(jnp.int32, (keys, queries), 0) <= lax.broadcasted_iota(
            jnp.int32, (keys, queries), 1
        )
    for head, (score, unit, start, size) in enumerate(
        ((score_b, broad_unit, 0, DB), (score_n, narrow_unit, DB, DN))
    ):
        if diagonal:
            score = jnp.where(allowed, score, -1e30)
            peak = jnp.max(score, axis=0, keepdims=True)
        else:
            peak = jnp.maximum(top[head], jnp.max(score, axis=0, keepdims=True))
        weight = jnp.exp2((score - peak) * unit)
        if diagonal:
            weight = jnp.where(allowed, weight, 0.0)
        added = jnp.sum(weight, axis=0, keepdims=True)
        product = dot(value_t[start : start + size], weight.astype(bf16))
        if diagonal:
            total[head] = added
            acc[start : start + size] = product
        else:
            factor = jnp.exp2((top[head] - peak) * unit)
            total[head] = total[head] * factor + added
            acc[start : start + size] = acc[start : start + size] * factor + product
        top[head] = peak


def ring_places(axis_size):
    return lambda at, step: lax.rem(at + step + axis_size, axis_size)


def offset_of(k):
    return (k + 1) // 2 * (1 if k % 2 else -1)


Y_BLOCKS = (0, -1, 1, 2)


def copies_of(nz, ny, crossed):
    assert ny == 4 and nz % 4 == 0
    last = nz // 2 - 1
    tasks = {}
    for d in (1, -1):
        tasks["ay", 0, d] = (("y", d), "a", 1, ())
        tasks["ay", 1, d] = (("y", d), "a" + "+-"[d < 0], 1, (("ay", 0, d),))
    source = {0: (), -1: (("ay", 0, 1),), 1: (("ay", 0, -1),), 2: (("ay", 1, 1), ("ay", 1, -1))}
    for s in range(last + 1):
        for j, at in enumerate(Y_BLOCKS):
            for d in (1, -1):
                if s < last or d == (1 if j % 2 == 0 else -1):
                    before = source[at] if s == 0 else (("az", s - 1, d, j),)
                    tasks["az", s, d, j] = (("z", d), "a", 1, before)
        for d in (1, -1):
            rows = "b" if s < last else "b" + "+-"[d < 0]
            tasks["bz", s, d] = (("z", d), rows, 1, () if s == 0 else (("bz", s - 1, d),))
    planes = {}
    for k in range(nz):
        off = offset_of(k)
        came = -1 if off > 0 else 1
        if k == 0:
            column, plane = (), tuple(tasks_ for tasks_ in tasks if tasks_[0] == "ay")
        elif k == nz - 1:
            column = (("bz", last, 1), ("bz", last, -1))
            plane = tuple(("az", last, 1 if j % 2 == 0 else -1, j) for j in range(ny)) + column
        else:
            column = (("bz", abs(off) - 1, came),)
            plane = tuple(("az", abs(off) - 1, came, j) for j in range(ny)) + column
        far = 1 if k % 2 == 0 else -1
        for d in (1, -1):
            tasks["by", k, 0, d] = (("y", d), "b", 1, column)
        tasks["by", k, 1, far] = (("y", far), "b", 1, (("by", k, 0, far),))
        plane += (("by", k, 0, 1), ("by", k, 0, -1), ("by", k, 1, far))
        if crossed:
            tasks["hand", k] = (("c", 0), "ab", ny, plane)
            given = (("hand", k),)
        else:
            round_y = ("ay", "az")
            for rows in "ab":
                parts = tuple(n for n in plane if (n[0] in round_y) == (rows == "a"))
                tasks["hand" + rows, k] = (("c", 0), rows, ny, parts)
            given = (("handa", k), ("handb", k))
        if crossed:
            if k == 0:
                blocks = (
                    (),
                    (("ay", 0, 1), ("by", 0, 0, 1)),
                    (("ay", 0, -1), ("by", 0, 0, -1)),
                    (("ay", 1, 1), ("ay", 1, -1), ("by", 0, 1, far)),
                )
                pieces = []
                for j, before in enumerate(blocks):
                    for d in (1, -1):
                        tasks["x0", j, d] = (("x", d), "x" + "+-"[d < 0] + "eo"[j % 2], 1, before)
                        pieces.append(("x0", j, d))
            else:
                pieces = [("x", k, 1), ("x", k, -1)]
                for d in (1, -1):
                    tasks["x", k, d] = (("x", d), "x", ny // 2, plane)
            pieces = tuple(pieces)
            tasks["handx", k] = (("c", 0), "x", ny, pieces)
            plane += (*pieces, ("handx", k))
        planes[k] = plane + given
    return tasks, planes


def foreseen(groups, delays, link_rate=43.5, chip_rate=450.0, latency=2.2):
    landed, waiting, free, now = {}, set(), {}, 0.0
    pending = []
    for g, (tasks, sizes) in groups.items():
        for name in tasks:
            waiting.add((g, name))
    started = set()

    def start_ready(time):
        for g, (tasks, sizes) in groups.items():
            if time < delays[g]:
                continue
            for name, (link, rows, blocks, before) in tasks.items():
                key = (g, name)
                if key in started or any((g, b) not in landed for b in before):
                    continue
                started.add(key)
                rate = chip_rate if link[0] == "c" else link_rate
                begin = max(time, free.get(link, 0.0))
                end = begin + sizes[rows] * blocks / rate / 1e3
                free[link] = end
                pending.append((end + (1.0 if link[0] == "c" else latency), key))

    times = sorted(set(delays.values()))
    while True:
        for t in times:
            if t <= now:
                start_ready(now)
        later = [t for t in times if t > now]
        upcoming = min(pending)[0] if pending else None
        if upcoming is None and not later:
            break
        if upcoming is None or (later and later[0] < upcoming):
            now = later[0]
            continue
        pending.sort()
        now, key = pending.pop(0)
        landed[key] = now
    return landed


class Web:
    def __init__(self, held, sems, place, tasks, cuts, crossed):
        self.held, self.sent, self.arrived = held, *sems
        self.z, self.y, self.core, self.x, self.parts = place
        self.nz, self.ny = held.shape[:2]
        self.tasks = tasks
        self.index = {name: i for i, name in enumerate(tasks)}
        a, b, a_cut, b_cut = cuts
        self.spans = {
            "a": (0, a),
            "b": (a, b),
            "a+": (0, a_cut),
            "a-": (a_cut, a - a_cut),
            "b+": (a, b_cut),
            "b-": (a + b_cut, b - b_cut),
            "ab": (0, a + b),
            "x": (0, a + b),
            "x+e": (0, (a + b) // 2),
            "x-e": ((a + b) // 2, (a + b) // 2),
            "x+o": (0, (a + b) // 2),
            "x-o": ((a + b) // 2, (a + b) // 2),
        }
        parity = lax.rem(self.x, 2) if crossed else 0
        self.base = parity * (a + b)
        self.other_base = (1 - parity) * (a + b)

    def sizes(self):
        row = self.held.shape[4] * 2
        return {key: size * row for key, (_, size) in self.spans.items()}

    def rows(self, key, base):
        start, size = self.spans[key]
        if isinstance(base, int):
            return pl.ds(base + start, size)
        return pl.ds(pl.multiple_of(base + start, 16), size)

    def device(self, z, y, core):
        return {"sp": (z * self.ny + y) * 2 + core}

    def copy(self, name):
        kind = name[0]
        link, key, _, _ = self.tasks[name]
        zs, ys, xs = ring_places(self.nz), ring_places(self.ny), ring_places(self.parts)
        z, y, c = self.z, self.y, self.core
        rows = self.rows(key, self.other_base if kind == "handx" else self.base)
        if kind == "ay":
            at = (z, ys(y, -name[1] * name[2]))
        elif kind == "az":
            at = (zs(z, -name[1] * name[2]), ys(y, Y_BLOCKS[name[3]]))
        elif kind == "bz":
            at = (zs(z, -name[1] * name[2]), y)
        elif kind == "by":
            at = (zs(z, offset_of(name[1])), ys(y, -name[2] * name[3]))
        elif kind == "x0":
            at = (z, ys(y, Y_BLOCKS[name[1]]))
        elif kind == "x":
            half = self.ny // 2
            at = (zs(z, offset_of(name[1])), pl.ds(0 if name[2] == 1 else half, half))
        else:
            at = (zs(z, offset_of(name[1])), pl.ds(0, self.ny))
        view = self.held.at[at[0], at[1], c, rows]
        axis, d = link
        to = {
            "y": lambda: self.device(z, ys(y, d), c),
            "z": lambda: self.device(zs(z, d), y, c),
            "c": lambda: self.device(z, y, 1 - c),
            "x": lambda: {"tp": xs(self.x, d)},
        }[axis]()
        i = self.index[name]
        return pltpu.make_async_remote_copy(
            src_ref=view,
            dst_ref=view,
            send_sem=self.sent.at[i],
            recv_sem=self.arrived.at[i],
            device_id=to,
            device_id_type=pl.DeviceIdType.MESH,
        )

    def drain(self):
        for name in self.tasks:
            self.copy(name).wait_send()


def program_of(webs, delays):
    times = foreseen({g: (web.tasks, web.sizes()) for g, web in webs.items()}, delays)
    seen, begun, lines = set(), set(), []

    def ready(group):
        names = [
            name
            for name, (_, _, _, before) in webs[group].tasks.items()
            if (group, name) not in begun and all((group, b) in seen for b in before)
        ]
        begun.update((group, name) for name in names)
        return [(group, name) for name in names]

    stops = [(delay, 0, group, None) for group, delay in delays.items()]
    stops += [(time, 1, group, name) for (group, name), time in times.items()]
    for time, _, group, name in sorted(stops, key=lambda s: (s[0], s[1], str(s[2:]))):
        if name is not None:
            seen.add((group, name))
        lines.append((time, None if name is None else (group, name), ready(group)))
    return lines, times


MESH = pl.DeviceIdType.MESH
CHUNK = 512
W_DELAY = 16.0
BLOCK_US = 1.6
LAG_US = 0.0


def layer_kernel(
    geometry,
    latent_hbm,
    q_broad,
    q_narrow,
    cosines,
    sines,
    key_cosines,
    key_sines,
    key_rope,
    latent_gain,
    key_up_broad,
    value_up_broad,
    key_up_narrow,
    value_up_narrow,
    post_gain,
    ffn_gain,
    ffn_out_gain,
    resid_hbm,
    out_broad_hbm,
    out_narrow_hbm,
    up_hbm,
    down_hbm,
    out,
    held,
    weights,
    all_q_broad,
    all_q_narrow,
    qt_broad,
    qt_narrow,
    w_key,
    w_value_t,
    top,
    total,
    acc,
    latent,
    rotated,
    broad_done,
    narrow_done,
    broad_theirs,
    narrow_theirs,
    gathered,
    out_broad,
    out_narrow,
    resid,
    wide,
    mixed,
    normed,
    hidden,
    partial,
    partial_sent,
    relayed,
    combined,
    from_far,
    from_near,
    local_sem,
    sent,
    arrived,
    w_sent,
    w_arrived,
    q_sent,
    q_arrived,
    a_sent,
    a_arrived,
    n_sent,
    n_arrived,
    r_sent,
    r_arrived,
):
    nz, ny, parts, cuts, w_cuts = geometry
    me, x = lax.axis_index("sp"), lax.axis_index("tp")
    core = lax.rem(me, 2)
    chip = me // 2
    z, y = chip // ny, lax.rem(chip, ny)
    rows = latent_hbm.shape[0]
    share = rows // parts
    zs, ys, xs = ring_places(nz), ring_places(ny), ring_places(parts)
    place = (z, y, core, x, parts)
    tasks, planes = copies_of(nz, ny, True)
    w_tasks, w_planes = copies_of(nz, ny, False)
    spread = Web(held, (sent, arrived), place, tasks, cuts, True)
    w_spread = Web(weights, (w_sent, w_arrived), place, w_tasks, w_cuts, False)
    webs = {"l": spread, "w": w_spread}
    lines, times = program_of(webs, {"l": 0.0, "w": W_DELAY})
    model_rows = up_hbm.shape[0]

    own_part = spread.rows("ab", spread.base)
    own_rows = pltpu.make_async_copy(latent_hbm.at[own_part], latent, local_sem.at[0])
    own_rows.start()
    loads = [
        (up_hbm, weights.at[z, y, core, pl.ds(0, model_rows)]),
        (down_hbm, weights.at[z, y, core, pl.ds(model_rows, model_rows)]),
        (out_broad_hbm, out_broad),
        (out_narrow_hbm, out_narrow),
        (resid_hbm, resid),
    ]
    loads = [
        pltpu.make_async_copy(src, dst, local_sem.at[i + 1]) for i, (src, dst) in enumerate(loads)
    ]
    for load in loads:
        load.start()

    right, left = {"tp": xs(x, 1)}, {"tp": xs(x, -1)}
    barrier = pltpu.get_barrier_semaphore()
    neighbours = [
        spread.device(z, y, 1 - core),
        spread.device(z, ys(y, 1), core),
        spread.device(z, ys(y, -1), core),
        spread.device(zs(z, 1), y, core),
        spread.device(zs(z, -1), y, core),
        right,
        left,
    ]
    for neighbour in neighbours:
        pl.semaphore_signal(barrier, inc=1, device_id=neighbour, device_id_type=MESH)

    tail = latent.shape[1]
    straight = dot(key_rope[...], picker((ROPE, 128), lambda r, k: r == k - ROPE), FIRST)
    swapped = dot(
        key_rope[...],
        picker(
            (ROPE, 128),
            lambda r, k: (k >= ROPE) & (r == jnp.where(k < ROPE + 32, k - 32, k - ROPE - 32)),
        ),
        FIRST,
    )
    rotated[...] = (straight * key_cosines[...] + swapped * key_sines[...]).astype(bf16)
    held[z, y, core, own_part, tail : tail + 128] = rotated[own_part, :]
    own_rows.wait()
    held[z, y, core, own_part, 0:tail] = rms_scale(latent[...].astype(f32), latent_gain[...]).astype(
        bf16
    )
    pl.semaphore_wait(barrier, len(neighbours))

    def carry_out(line):
        _, landing, starts = line
        if landing is not None:
            webs[landing[0]].copy(landing[1]).wait_recv()
        for group, name in starts:
            webs[group].copy(name).start()

    carry_out(lines.pop(0))

    def remote(src, dst, sems, i, device):
        return pltpu.make_async_remote_copy(
            src_ref=src,
            dst_ref=dst,
            send_sem=sems[0].at[i],
            recv_sem=sems[1].at[i],
            device_id=device,
            device_id_type=MESH,
        )

    partner = spread.device(z, y, 1 - core)
    q_sems, a_sems, n_sems, r_sems = (
        (q_sent, q_arrived),
        (a_sent, a_arrived),
        (n_sent, n_arrived),
        (r_sent, r_arrived),
    )
    exchange = [
        remote(q_broad, all_q_broad.at[core], q_sems, 0, partner),
        remote(q_narrow, all_q_narrow.at[core], q_sems, 1, partner),
    ]
    for copy in exchange:
        copy.start()
    all_q_broad[core] = q_broad[...]
    all_q_narrow[core] = q_narrow[...]
    for copy in exchange:
        copy.wait_recv()
    prepare(
        core,
        all_q_broad[...].reshape(2 * rows, -1),
        all_q_narrow[...].reshape(2 * rows, -1),
        cosines[...],
        sines[...],
        (key_up_broad, value_up_broad, key_up_narrow, value_up_narrow),
        qt_broad,
        qt_narrow,
        w_key,
        w_value_t,
    )
    for load in loads:
        load.wait()
    ready = [max(times["l", name] for name in planes[k]) for k in range(nz)]

    def carry_out_until(time):
        while lines and lines[0][0] <= time:
            carry_out(lines.pop(0))

    carry_out_until(ready[0])
    tools = (qt_broad, qt_narrow, w_key, w_value_t, top, total, acc)

    def block_of(at_z, at_y):
        return held[at_z, at_y].reshape(2 * rows, -1)

    attend_block(block_of(z, y), True, *tools)

    @pl.when(lax.rem(y, 2) == 1)
    def _():
        attend_block(block_of(z, y - 1), False, *tools)


    turns, clock = {}, ready[0] + 2.0
    steps = nz * ny // 2
    for step in range(steps):
        clock = max(clock, ready[step // (ny // 2)])
        while lines and lines[0][0] <= clock + LAG_US:
            turns.setdefault(step, []).append(lines.pop(0))
        clock += BLOCK_US

    def earlier(step, carried):
        for turn, due in turns.items():

            @pl.when(step == turn)
            def _(due=due):
                for line in due:
                    carry_out(line)

        k = step // (ny // 2)
        half = (k + 1) // 2
        at_z = zs(z, half * (2 * lax.rem(k, 2) - 1))
        at_y = 2 * lax.rem(step, ny // 2)

        @pl.when(at_z * ny + at_y + 1 < chip)
        def _():
            attend_block(held[at_z, pl.ds(at_y, 2)].reshape(4 * rows, -1), False, *tools)

        return carried

    lax.fori_loop(0, steps, earlier, 0)

    broad_done[...] = jnp.transpose(acc[0:DB] / total[0]).astype(bf16).reshape(2, rows, DB)
    narrow_done[...] = (
        jnp.transpose(acc[DB : DB + DN] / total[1]).astype(bf16).reshape(2, rows, DN)
    )
    swap = [
        remote(broad_done.at[1 - core], broad_theirs, a_sems, 0, partner),
        remote(narrow_done.at[1 - core], narrow_theirs, a_sems, 1, partner),
    ]
    for copy in swap:
        copy.start()
    carry_out_until(clock + 1.5)
    for copy in swap:
        copy.wait_recv()
    pairs = [
        (mine, theirs[...])
        for mine, theirs in (
            (broad_done[core], broad_theirs),
            (narrow_done[core], narrow_theirs),
        )
    ]
    gathered[x] = jnp.concatenate(
        [half for mine, theirs in pairs for half in (
            jnp.where(core == 0, mine, theirs), jnp.where(core == 0, theirs, mine)
        )],
        axis=1,
    )
    halves = (pl.ds(0, rows // 2), pl.ds(rows // 2, rows // 2))

    def along_x(at, half, i, device):
        view = gathered.at[at, halves[half]]
        return remote(view, view, n_sems, i, device)

    around = [
        along_x(x, 0, 0, right),
        along_x(x, 1, 1, left),
        along_x(x, 1, 2, right),
        along_x(x, 0, 3, left),
        along_x(xs(x, -1), 0, 4, right),
        along_x(xs(x, 1), 1, 5, left),
    ]
    for copy in around[:4]:
        copy.start()
    spread.drain()
    carry_out_until(clock + 5.0)
    around[0].wait_recv()
    around[4].start()
    around[1].wait_recv()
    around[5].start()
    carry_out_until(clock + 9.0)
    for copy in around[2:]:
        copy.wait_recv()
    rows_broad = jnp.concatenate([gathered[i, :, 0 : 2 * DB] for i in range(parts)], axis=1)
    rows_narrow = jnp.concatenate(
        [gathered[i, :, 2 * DB : 2 * (DB + DN)] for i in range(parts)], axis=1
    )
    width = out.shape[1]

    def project(n, carried):
        columns = pl.ds(pl.multiple_of(n * CHUNK, CHUNK), CHUNK)
        wide[:, columns] = dot(rows_broad, out_broad[:, columns]) + dot(
            rows_narrow, out_narrow[:, columns]
        )
        return carried

    lax.fori_loop(0, width // CHUNK, project, 0)

    def norm_share(i, carried):
        at = pl.ds(pl.multiple_of(i * share, 16), share)
        mix = (resid[at].astype(f32) + rms_scale(wide[at], post_gain[...])).astype(bf16)
        mixed[i] = mix
        normed[i] = rms_scale(mix.astype(f32), ffn_gain[...]).astype(bf16)
        return carried

    lax.fori_loop(0, parts, norm_share, 0)
    inputs = normed[...].reshape(rows, width)
    carry_out_until(
        max(times["w", n] for k in range(nz) for n in w_planes[k] if n[0] in ("ay", "az", "handa"))
    )

    def raise_up(n, carried):
        columns = pl.ds(pl.multiple_of(n * CHUNK, CHUNK), CHUNK)
        up = weights[:, :, :, 0:model_rows, columns].reshape(width, CHUNK)
        raised = jnp.maximum(dot(inputs, up), 0.0)
        hidden[:, columns] = (raised * raised).astype(bf16)
        return carried

    lax.fori_loop(0, hidden.shape[1] // CHUNK, raise_up, 0)
    while lines:
        carry_out(lines.pop(0))

    pieces = width // CHUNK
    per_z = 2 * ny * model_rows
    copies = {}
    for n in range(pieces):
        d = 1 if n % 2 == 0 else -1
        columns = slice(n * CHUNK, (n + 1) * CHUNK)
        near, far = {"tp": xs(x, d)}, {"tp": xs(x, -d)}
        copies[n] = (
            remote(partial_sent.at[xs(x, 2), :, columns], relayed.at[n], r_sems, 3 * n, near),
            remote(
                partial_sent.at[xs(x, -d), :, columns],
                from_near.at[:, columns],
                r_sems,
                3 * n + 1,
                far,
            ),
            remote(combined.at[n], from_far.at[:, columns], r_sems, 3 * n + 2, near),
        )

    def lower(n):
        columns = slice(n * CHUNK, (n + 1) * CHUNK)
        zn = CHUNK // per_z
        down = weights[n * zn : (n + 1) * zn, :, :, model_rows : 2 * model_rows].reshape(
            CHUNK, hidden.shape[1]
        )
        sums = dot(hidden[...], down, LAST).reshape(parts, share, CHUNK)
        partial[:, :, columns] = sums
        partial_sent[:, :, columns] = sums.astype(bf16)
        copies[n][0].start()
        copies[n][1].start()

    def relay(n):
        d = 1 if n % 2 == 0 else -1
        columns = slice(n * CHUNK, (n + 1) * CHUNK)
        copies[n][0].wait_recv()
        combined[n] = (partial[xs(x, d), :, columns] + relayed[n].astype(f32)).astype(bf16)
        copies[n][2].start()

    for n in range(pieces):
        lower(n)
    for n in range(pieces):
        relay(n)
    w_spread.drain()
    for copy in exchange + swap + around:
        copy.wait_send()
    for n in range(pieces):
        copies[n][1].wait_recv()
        copies[n][2].wait_recv()
    ffn = partial[x] + from_near[...].astype(f32) + from_far[...].astype(f32)
    out[...] = (mixed[x].astype(f32) + rms_scale(ffn, ffn_out_gain[...])).astype(bf16)
    for n in range(pieces):
        for copy in copies[n]:
            copy.wait_send()


def rms_scale(values, norm_gain):
    return (
        values * lax.rsqrt(jnp.mean(values * values, axis=-1, keepdims=True) + norm_eps) * norm_gain
    )


def layer(geometry, latent, queries, tables, key_rope, ups, gains, resid, outs, up_weight, down_weight):
    nz, ny, parts = geometry[:3]
    rows, latent_width = latent.shape
    width = resid.shape[1]
    hidden = up_weight.shape[1]
    share = rows // parts
    model_rows = up_weight.shape[0]
    vmem = pl.BlockSpec(memory_space=pltpu.VMEM)
    anywhere = pl.BlockSpec(memory_space=pl.ANY)
    copies = len(copies_of(nz, ny, True)[0])
    w_copies = len(copies_of(nz, ny, False)[0])
    pieces = width // CHUNK
    sems = pltpu.SemaphoreType.DMA
    operands = (
        latent,
        *queries,
        *tables,
        key_rope,
        gains[0],
        *ups,
        *gains[1:],
        resid,
        *outs,
        up_weight,
        down_weight,
    )
    return pl.pallas_call(
        functools.partial(layer_kernel, geometry),
        out_shape=jax.ShapeDtypeStruct((share, width), bf16),
        in_specs=[anywhere] + [vmem] * 15 + [anywhere] * 5,
        out_specs=vmem,
        scratch_shapes=[
            pltpu.VMEM((nz, ny, 2, rows, latent_width + 128), bf16),
            pltpu.VMEM((nz, ny, 2, 2 * model_rows, hidden), bf16),
            pltpu.VMEM((2, rows, queries[0].shape[1]), bf16),
            pltpu.VMEM((2, rows, queries[1].shape[1]), bf16),
            pltpu.VMEM((256, 2 * rows), bf16),
            pltpu.VMEM((128, 2 * rows), bf16),
            pltpu.VMEM((512, 256), bf16),
            pltpu.VMEM((DB + DN, 512), bf16),
            pltpu.VMEM((2, 1, 2 * rows), f32),
            pltpu.VMEM((2, 1, 2 * rows), f32),
            pltpu.VMEM((DB + DN, 2 * rows), f32),
            pltpu.VMEM((rows // 2, latent_width), bf16),
            pltpu.VMEM((rows, 128), bf16),
            pltpu.VMEM((2, rows, DB), bf16),
            pltpu.VMEM((2, rows, DN), bf16),
            pltpu.VMEM((rows, DB), bf16),
            pltpu.VMEM((rows, DN), bf16),
            pltpu.VMEM((parts, rows, 2 * (DB + DN)), bf16),
            pltpu.VMEM(outs[0].shape, bf16),
            pltpu.VMEM(outs[1].shape, bf16),
            pltpu.VMEM((rows, width), bf16),
            pltpu.VMEM((rows, width), f32),
            pltpu.VMEM((parts, share, width), bf16),
            pltpu.VMEM((parts, share, width), bf16),
            pltpu.VMEM((rows, hidden), bf16),
            pltpu.VMEM((parts, share, width), f32),
            pltpu.VMEM((parts, share, width), bf16),
            pltpu.VMEM((pieces, share, CHUNK), bf16),
            pltpu.VMEM((pieces, share, CHUNK), bf16),
            pltpu.VMEM((share, width), bf16),
            pltpu.VMEM((share, width), bf16),
            sems((6,)),
            sems((copies,)),
            sems((copies,)),
            sems((w_copies,)),
            sems((w_copies,)),
            sems((2,)),
            sems((2,)),
            sems((2,)),
            sems((2,)),
            sems((6,)),
            sems((6,)),
            sems((3 * pieces,)),
            sems((3 * pieces,)),
        ],
        compiler_params=pltpu.CompilerParams(
            collective_id=0, has_side_effects=True, vmem_limit_bytes=63 * 1024 * 1024
        ),
        cost_estimate=pl.CostEstimate(
            flops=40_000_000_000, bytes_accessed=20_000_000, transcendentals=9_000_000
        ),
        name="layer",
    )(*operands)


def frequency_of(lane):
    return rope_base ** (-2.0 * lax.rem(lane, ROPE // 2).astype(f32) / ROPE)


def local(
    resid,
    query_broad,
    query_narrow,
    latent,
    key_rope,
    latent_gain,
    key_up_broad,
    value_up_broad,
    key_up_narrow,
    value_up_narrow,
    out_broad,
    out_narrow,
    post_gain,
    ffn_gain,
    up_weight,
    down_weight,
    ffn_out_gain,
):
    rows = resid.shape[0]
    parts = lax.axis_size("tp")
    me = lax.axis_index("sp")
    nz = lax.axis_size("sp") // (2 * NY)

    lane = jnp.arange(128, dtype=jnp.int32)
    positions = (me * rows + jnp.arange(rows, dtype=jnp.int32)).astype(f32)
    angles = positions[:, None] * frequency_of(lane)[None, :]
    sign = jnp.where(lane < ROPE, 0.0, jnp.where(lane < ROPE + ROPE // 2, -1.0, 1.0))
    key_cosines = jnp.cos(angles) * (sign * sign)[None, :]
    key_sines = jnp.sin(angles) * sign[None, :]
    lane = jnp.arange(ROPE, dtype=jnp.int32)
    positions = ((me // 2) * 2 * rows + jnp.arange(2 * rows, dtype=jnp.int32)).astype(f32)
    angles = frequency_of(lane)[:, None] * positions[None, :]
    cosines = jnp.cos(angles)
    sines = jnp.sin(angles) * jnp.where(lane < ROPE // 2, -1.0, 1.0)[:, None]
    return layer(
        (nz, NY, parts, (32, 64, 16, 32), (32, 32, 16, 16)),
        latent,
        (query_broad, query_narrow),
        (cosines, sines, key_cosines, key_sines),
        key_rope.T,
        (key_up_broad, value_up_broad, key_up_narrow, value_up_narrow),
        (latent_gain[None, :], post_gain[None, :], ffn_gain[None, :], ffn_out_gain[None, :]),
        resid,
        (out_broad, out_narrow),
        up_weight,
        down_weight,
    )


def solution(mesh):
    in_specs = (
        P("sp", None),
        P("sp", "tp"),
        P("sp", "tp"),
        P("sp", None),
        P("sp", None),
        P(),
        P(None, "tp"),
        P(None, "tp"),
        P(None, "tp"),
        P(None, "tp"),
        P(),
        P(),
        P(),
        P(),
        P("sp", "tp"),
        P("sp", "tp"),
        P(),
    )
    out_specs = P(("sp", "tp"), None)
    return jax.shard_map(local, mesh=mesh, in_specs=in_specs, out_specs=out_specs, check_vma=False)
```

```python
import functools
import math

import jax
import jax.numpy as jnp
from jax import lax
from jax.experimental import pallas as pl
from jax.experimental.pallas import tpu as pltpu
from jax.sharding import PartitionSpec as P

DB = 128
DN = 64
ROPE = 64
NY = 4

norm_eps = 1e-06
rope_base = 500000.0
broad_unit = (DB + ROPE) ** (-0.5) * math.log2(math.e)
narrow_unit = (DN + ROPE) ** (-0.5) * math.log2(math.e)
f32 = jnp.float32
bf16 = jnp.bfloat16


def dot(a, b, dims=((1,), (0,))):
    return lax.dot_general(a, b, (dims, ((), ())), preferred_element_type=f32)


def picker(shape, pick):
    rows = lax.broadcasted_iota(jnp.int32, shape, 0)
    columns = lax.broadcasted_iota(jnp.int32, shape, 1)
    return jnp.where(pick(rows, columns), 1.0, 0.0).astype(bf16)


LAST = ((1,), (1,))
FIRST = ((0,), (0,))


def prepare(core, q_broad, q_narrow, cosines, sines, refs, qt_broad, qt_narrow, w_key, w_value_t):
    key_up_broad, value_up_broad, key_up_narrow, value_up_narrow = refs
    at = core * (DB + ROPE)
    rows = q_broad.shape[0]
    wide = q_broad.shape[1]
    qt_broad[0:DB] = dot(
        picker((DB, wide), lambda r, k: k == r + at), q_broad, LAST
    ).astype(bf16)
    qt_broad[DB : DB + 64] = jnp.zeros((64, rows), bf16)

    def rotated(value, start):
        straight = dot(picker((64, value.shape[1]), lambda r, k: k == r + start), value, LAST)
        swapped = dot(
            picker(
                (64, value.shape[1]), lambda r, k: k == jnp.where(r < 32, r + 32, r - 32) + start
            ),
            value,
            LAST,
        )
        return (straight * cosines + swapped * sines).astype(bf16)

    qt_broad[DB + 64 : DB + 128] = rotated(q_broad, at + DB)
    at_n = core * (DN + ROPE)
    qt_narrow[0:64] = dot(
        picker((64, q_narrow.shape[1]), lambda r, k: k == r + at_n), q_narrow, LAST
    ).astype(bf16)
    qt_narrow[64:128] = rotated(q_narrow, at_n + DN)
    w_key[:, 0:DB] = key_up_broad[:, pl.ds(pl.multiple_of(core * DB, DB), DB)]
    w_key[:, DB : DB + 128] = dot(
        key_up_narrow[...], picker((128, 128), lambda r, k: (r == k + core * DN) & (k < DN))
    ).astype(bf16)
    w_value_t[0:DB] = dot(
        picker((DB, 2 * DB), lambda r, k: k == r + core * DB), value_up_broad[...], LAST
    ).astype(bf16)
    w_value_t[DB : DB + DN] = dot(
        picker((DN, 2 * DN), lambda r, k: k == r + core * DN), value_up_narrow[...], LAST
    ).astype(bf16)


def attend_block(block, diagonal, qt_broad, qt_narrow, w_key, w_value_t, top, total, acc):
    keys, queries = block.shape[0], qt_broad.shape[1]
    latent = block[:, 0:512]
    expanded = dot(latent, w_key[...])
    key_b = expanded[:, 0:DB].astype(bf16)
    key_n = (expanded[:, DB : DB + 128] + block[:, 512:640].astype(f32)).astype(bf16)
    value_t = dot(w_value_t[...], latent, LAST).astype(bf16)
    score_b = dot(jnp.concatenate([key_b, key_n], axis=1), qt_broad[...])
    score_n = dot(key_n, qt_narrow[...])
    if diagonal:
        allowed = lax.broadcasted_iota(jnp.int32, (keys, queries), 0) <= lax.broadcasted_iota(
            jnp.int32, (keys, queries), 1
        )
    for head, (score, unit, start, size) in enumerate(
        ((score_b, broad_unit, 0, DB), (score_n, narrow_unit, DB, DN))
    ):
        if diagonal:
            score = jnp.where(allowed, score, -1e30)
            peak = jnp.max(score, axis=0, keepdims=True)
        else:
            peak = jnp.maximum(top[head], jnp.max(score, axis=0, keepdims=True))
        weight = jnp.exp2((score - peak) * unit)
        if diagonal:
            weight = jnp.where(allowed, weight, 0.0)
        added = jnp.sum(weight, axis=0, keepdims=True)
        product = dot(value_t[start : start + size], weight.astype(bf16))
        if diagonal:
            total[head] = added
            acc[start : start + size] = product
        else:
            factor = jnp.exp2((top[head] - peak) * unit)
            total[head] = total[head] * factor + added
            acc[start : start + size] = acc[start : start + size] * factor + product
        top[head] = peak


def ring_places(axis_size):
    return lambda at, step: lax.rem(at + step + axis_size, axis_size)


def offset_of(k):
    return (k + 1) // 2 * (1 if k % 2 else -1)


Y_BLOCKS = (0, -1, 1, 2)


def copies_of(nz, ny, crossed):
    assert ny == 4 and nz % 4 == 0
    last = nz // 2 - 1
    tasks = {}
    for d in (1, -1):
        tasks["ay", 0, d] = (("y", d), "a", 1, ())
        tasks["ay", 1, d] = (("y", d), "a" + "+-"[d < 0], 1, (("ay", 0, d),))
    source = {0: (), -1: (("ay", 0, 1),), 1: (("ay", 0, -1),), 2: (("ay", 1, 1), ("ay", 1, -1))}
    for s in range(last + 1):
        for j, at in enumerate(Y_BLOCKS):
            for d in (1, -1):
                if s < last or d == (1 if j % 2 == 0 else -1):
                    before = source[at] if s == 0 else (("az", s - 1, d, j),)
                    tasks["az", s, d, j] = (("z", d), "a", 1, before)
        for d in (1, -1):
            rows = "b" if s < last else "b" + "+-"[d < 0]
            tasks["bz", s, d] = (("z", d), rows, 1, () if s == 0 else (("bz", s - 1, d),))
    planes = {}
    for k in range(nz):
        off = offset_of(k)
        came = -1 if off > 0 else 1
        if k == 0:
            column, plane = (), tuple(tasks_ for tasks_ in tasks if tasks_[0] == "ay")
        elif k == nz - 1:
            column = (("bz", last, 1), ("bz", last, -1))
            plane = tuple(("az", last, 1 if j % 2 == 0 else -1, j) for j in range(ny)) + column
        else:
            column = (("bz", abs(off) - 1, came),)
            plane = tuple(("az", abs(off) - 1, came, j) for j in range(ny)) + column
        far = 1 if k % 2 == 0 else -1
        for d in (1, -1):
            tasks["by", k, 0, d] = (("y", d), "b", 1, column)
        tasks["by", k, 1, far] = (("y", far), "b", 1, (("by", k, 0, far),))
        plane += (("by", k, 0, 1), ("by", k, 0, -1), ("by", k, 1, far))
        tasks["hand", k] = (("c", 0), "ab", ny, plane)
        if crossed:
            if k == 0:
                blocks = (
                    (),
                    (("ay", 0, 1), ("by", 0, 0, 1)),
                    (("ay", 0, -1), ("by", 0, 0, -1)),
                    (("ay", 1, 1), ("ay", 1, -1), ("by", 0, 1, far)),
                )
                pieces = []
                for j, before in enumerate(blocks):
                    for d in (1, -1):
                        tasks["x0", j, d] = (("x", d), "x" + "+-"[d < 0] + "eo"[j % 2], 1, before)
                        pieces.append(("x0", j, d))
            else:
                pieces = [("x", k, 1), ("x", k, -1)]
                for d in (1, -1):
                    tasks["x", k, d] = (("x", d), "x", ny // 2, plane)
            pieces = tuple(pieces)
            tasks["handx", k] = (("c", 0), "x", ny, pieces)
            plane += (*pieces, ("handx", k))
        planes[k] = plane + (("hand", k),)
    return tasks, planes


def foreseen(groups, delays, link_rate=43.5, chip_rate=450.0, latency=2.2):
    landed, waiting, free, now = {}, set(), {}, 0.0
    pending = []
    for g, (tasks, sizes) in groups.items():
        for name in tasks:
            waiting.add((g, name))
    started = set()

    def start_ready(time):
        for g, (tasks, sizes) in groups.items():
            if time < delays[g]:
                continue
            for name, (link, rows, blocks, before) in tasks.items():
                key = (g, name)
                if key in started or any((g, b) not in landed for b in before):
                    continue
                started.add(key)
                rate = chip_rate if link[0] == "c" else link_rate
                begin = max(time, free.get(link, 0.0))
                end = begin + sizes[rows] * blocks / rate / 1e3
                free[link] = end
                pending.append((end + (1.0 if link[0] == "c" else latency), key))

    times = sorted(set(delays.values()))
    while True:
        for t in times:
            if t <= now:
                start_ready(now)
        later = [t for t in times if t > now]
        upcoming = min(pending)[0] if pending else None
        if upcoming is None and not later:
            break
        if upcoming is None or (later and later[0] < upcoming):
            now = later[0]
            continue
        pending.sort()
        now, key = pending.pop(0)
        landed[key] = now
    return landed


class Web:
    def __init__(self, held, sems, place, tasks, spans, crossed):
        self.held, self.sent, self.arrived = held, *sems
        self.z, self.y, self.core, self.x, self.parts = place
        self.nz, self.ny = held.shape[:2]
        self.tasks = tasks
        self.index = {name: i for i, name in enumerate(tasks)}
        self.spans = spans
        self.count = spans["ab"][1]
        parity = lax.rem(self.x, 2) if crossed else 0
        self.base = parity * self.count
        self.other_base = (1 - parity) * self.count

    def sizes(self):
        return {
            key: rows * columns * 2 * (rows > 0) for key, (_, rows, _, columns) in self.spans.items()
        }

    def part(self, key, base):
        start, rows, first, columns = self.spans[key]
        at = base + start
        if not isinstance(base, int):
            at = pl.multiple_of(at, 16)
        return pl.ds(at, rows), pl.ds(first, columns)

    def device(self, z, y, core):
        return {"sp": (z * self.ny + y) * 2 + core}

    def copy(self, name):
        kind = name[0]
        link, key, _, _ = self.tasks[name]
        zs, ys, xs = ring_places(self.nz), ring_places(self.ny), ring_places(self.parts)
        z, y, c = self.z, self.y, self.core
        rows, columns = self.part(key, self.other_base if kind == "handx" else self.base)
        if kind == "ay":
            at = (z, ys(y, -name[1] * name[2]))
        elif kind == "az":
            at = (zs(z, -name[1] * name[2]), ys(y, Y_BLOCKS[name[3]]))
        elif kind == "bz":
            at = (zs(z, -name[1] * name[2]), y)
        elif kind == "by":
            at = (zs(z, offset_of(name[1])), ys(y, -name[2] * name[3]))
        elif kind == "x0":
            at = (z, ys(y, Y_BLOCKS[name[1]]))
        elif kind == "x":
            half = self.ny // 2
            at = (zs(z, offset_of(name[1])), pl.ds(0 if name[2] == 1 else half, half))
        else:
            at = (zs(z, offset_of(name[1])), pl.ds(0, self.ny))
        view = self.held.at[at[0], at[1], c, rows, columns]
        axis, d = link
        to = {
            "y": lambda: self.device(z, ys(y, d), c),
            "z": lambda: self.device(zs(z, d), y, c),
            "c": lambda: self.device(z, y, 1 - c),
            "x": lambda: {"tp": xs(self.x, d)},
        }[axis]()
        i = self.index[name]
        return pltpu.make_async_remote_copy(
            src_ref=view,
            dst_ref=view,
            send_sem=self.sent.at[i],
            recv_sem=self.arrived.at[i],
            device_id=to,
            device_id_type=pl.DeviceIdType.MESH,
        )

    def drain(self):
        for name in self.tasks:
            self.copy(name).wait_send()


def split_rows(a, b, a_cut, b_cut, columns):
    half = (a + b) // 2
    rows = {
        "a": (0, a),
        "b": (a, b),
        "a+": (0, a_cut),
        "a-": (a_cut, a - a_cut),
        "b+": (a, b_cut),
        "b-": (a + b_cut, b - b_cut),
        "ab": (0, a + b),
        "x": (0, a + b),
        "x+e": (0, half),
        "x-e": (half, half),
        "x+o": (0, half),
        "x-o": (half, half),
    }
    return {key: (*span, 0, columns) for key, span in rows.items()}


def split_columns(rows, cut, columns):
    half = rows // 2
    spans = {"ab": (0, rows, 0, columns)}
    for key, first, size in (("a", 0, cut), ("b", cut, columns - cut)):
        spans[key] = (0, rows, first, size)
        spans[key + "+"] = (0, half, first, size)
        spans[key + "-"] = (half, half, first, size)
    return spans


def program_of(webs, delays):
    times = foreseen({g: (web.tasks, web.sizes()) for g, web in webs.items()}, delays)
    seen, begun, lines = set(), set(), []

    def ready(group):
        names = [
            name
            for name, (_, _, _, before) in webs[group].tasks.items()
            if (group, name) not in begun and all((group, b) in seen for b in before)
        ]
        begun.update((group, name) for name in names)
        return [(group, name) for name in names]

    stops = [(delay, 0, group, None) for group, delay in delays.items()]
    stops += [(time, 1, group, name) for (group, name), time in times.items()]
    for time, _, group, name in sorted(stops, key=lambda s: (s[0], s[1], str(s[2:]))):
        if name is not None:
            seen.add((group, name))
        lines.append((time, None if name is None else (group, name), ready(group)))
    return lines, times


MESH = pl.DeviceIdType.MESH
CHUNK = 512
UP_DELAY = 10.0
DOWN_DELAY = 20.0
W_CUT = 896
L_CUTS = (32, 64, 16, 32)
BLOCK_US = 1.6
LAG_US = 0.0


def layer_kernel(
    geometry,
    latent_hbm,
    q_broad,
    q_narrow,
    cosines,
    sines,
    key_cosines,
    key_sines,
    key_rope,
    latent_gain,
    key_up_broad,
    value_up_broad,
    key_up_narrow,
    value_up_narrow,
    post_gain,
    ffn_gain,
    ffn_out_gain,
    resid_hbm,
    out_broad_hbm,
    out_narrow_hbm,
    up_hbm,
    down_hbm,
    out,
    held,
    up_held,
    down_held,
    all_q_broad,
    all_q_narrow,
    qt_broad,
    qt_narrow,
    w_key,
    w_value_t,
    top,
    total,
    acc,
    latent,
    rotated,
    broad_done,
    narrow_done,
    broad_theirs,
    narrow_theirs,
    gathered,
    out_broad,
    out_narrow,
    resid,
    wide,
    mixed,
    normed,
    hidden,
    partial,
    partial_sent,
    relayed,
    combined,
    from_far,
    from_near,
    local_sem,
    sent,
    arrived,
    up_sent,
    up_arrived,
    down_sent,
    down_arrived,
    q_sent,
    q_arrived,
    a_sent,
    a_arrived,
    n_sent,
    n_arrived,
    r_sent,
    r_arrived,
):
    nz, ny, parts = geometry
    me, x = lax.axis_index("sp"), lax.axis_index("tp")
    core = lax.rem(me, 2)
    chip = me // 2
    z, y = chip // ny, lax.rem(chip, ny)
    rows = latent_hbm.shape[0]
    share = rows // parts
    zs, ys, xs = ring_places(nz), ring_places(ny), ring_places(parts)
    place = (z, y, core, x, parts)
    tasks, planes = copies_of(nz, ny, True)
    w_tasks, w_planes = copies_of(nz, ny, False)
    model_rows, w_columns = up_hbm.shape
    w_spans = split_columns(model_rows, W_CUT, w_columns)
    spread = Web(held, (sent, arrived), place, tasks, split_rows(*L_CUTS, held.shape[4]), True)
    up_web = Web(up_held, (up_sent, up_arrived), place, w_tasks, w_spans, False)
    down_web = Web(down_held, (down_sent, down_arrived), place, w_tasks, w_spans, False)
    webs = {"l": spread, "u": up_web, "w": down_web}
    lines, times = program_of(webs, {"l": 0.0, "u": UP_DELAY, "w": DOWN_DELAY})

    own_part, _ = spread.part("ab", spread.base)
    own_rows = pltpu.make_async_copy(latent_hbm.at[own_part], latent, local_sem.at[0])
    own_rows.start()
    loads = [
        (up_hbm, up_held.at[z, y, core]),
        (down_hbm, down_held.at[z, y, core]),
        (out_broad_hbm, out_broad),
        (out_narrow_hbm, out_narrow),
        (resid_hbm, resid),
    ]
    loads = [
        pltpu.make_async_copy(src, dst, local_sem.at[i + 1]) for i, (src, dst) in enumerate(loads)
    ]
    for load in loads:
        load.start()

    right, left = {"tp": xs(x, 1)}, {"tp": xs(x, -1)}
    barrier = pltpu.get_barrier_semaphore()
    neighbours = [
        spread.device(z, y, 1 - core),
        spread.device(z, ys(y, 1), core),
        spread.device(z, ys(y, -1), core),
        spread.device(zs(z, 1), y, core),
        spread.device(zs(z, -1), y, core),
        right,
        left,
    ]
    for neighbour in neighbours:
        pl.semaphore_signal(barrier, inc=1, device_id=neighbour, device_id_type=MESH)

    tail = latent.shape[1]
    straight = dot(key_rope[...], picker((ROPE, 128), lambda r, k: r == k - ROPE), FIRST)
    swapped = dot(
        key_rope[...],
        picker(
            (ROPE, 128),
            lambda r, k: (k >= ROPE) & (r == jnp.where(k < ROPE + 32, k - 32, k - ROPE - 32)),
        ),
        FIRST,
    )
    rotated[...] = (straight * key_cosines[...] + swapped * key_sines[...]).astype(bf16)
    held[z, y, core, own_part, tail : tail + 128] = rotated[own_part, :]
    own_rows.wait()
    held[z, y, core, own_part, 0:tail] = rms_scale(latent[...].astype(f32), latent_gain[...]).astype(
        bf16
    )
    pl.semaphore_wait(barrier, len(neighbours))

    def carry_out(line):
        _, landing, starts = line
        if landing is not None:
            webs[landing[0]].copy(landing[1]).wait_recv()
        for group, name in starts:
            webs[group].copy(name).start()

    carry_out(lines.pop(0))

    def remote(src, dst, sems, i, device):
        return pltpu.make_async_remote_copy(
            src_ref=src,
            dst_ref=dst,
            send_sem=sems[0].at[i],
            recv_sem=sems[1].at[i],
            device_id=device,
            device_id_type=MESH,
        )

    partner = spread.device(z, y, 1 - core)
    q_sems, a_sems, n_sems, r_sems = (
        (q_sent, q_arrived),
        (a_sent, a_arrived),
        (n_sent, n_arrived),
        (r_sent, r_arrived),
    )
    exchange = [
        remote(q_broad, all_q_broad.at[core], q_sems, 0, partner),
        remote(q_narrow, all_q_narrow.at[core], q_sems, 1, partner),
    ]
    for copy in exchange:
        copy.start()
    all_q_broad[core] = q_broad[...]
    all_q_narrow[core] = q_narrow[...]
    for copy in exchange:
        copy.wait_recv()
    prepare(
        core,
        all_q_broad[...].reshape(2 * rows, -1),
        all_q_narrow[...].reshape(2 * rows, -1),
        cosines[...],
        sines[...],
        (key_up_broad, value_up_broad, key_up_narrow, value_up_narrow),
        qt_broad,
        qt_narrow,
        w_key,
        w_value_t,
    )
    for load in loads:
        load.wait()
    ready = [max(times["l", name] for name in planes[k]) for k in range(nz)]

    def carry_out_until(time):
        while lines and lines[0][0] <= time:
            carry_out(lines.pop(0))

    carry_out_until(ready[0])
    tools = (qt_broad, qt_narrow, w_key, w_value_t, top, total, acc)

    def block_of(at_z, at_y):
        return held[at_z, at_y].reshape(2 * rows, -1)

    attend_block(block_of(z, y), True, *tools)

    @pl.when(lax.rem(y, 2) == 1)
    def _():
        attend_block(block_of(z, y - 1), False, *tools)


    turns, clock = {}, ready[0] + 2.0
    steps = nz * ny // 2
    for step in range(steps):
        clock = max(clock, ready[step // (ny // 2)])
        while lines and lines[0][0] <= clock + LAG_US:
            turns.setdefault(step, []).append(lines.pop(0))
        clock += BLOCK_US

    def earlier(step, carried):
        for turn, due in turns.items():

            @pl.when(step == turn)
            def _(due=due):
                for line in due:
                    carry_out(line)

        k = step // (ny // 2)
        half = (k + 1) // 2
        at_z = zs(z, half * (2 * lax.rem(k, 2) - 1))
        at_y = 2 * lax.rem(step, ny // 2)

        @pl.when(at_z * ny + at_y + 1 < chip)
        def _():
            attend_block(held[at_z, pl.ds(at_y, 2)].reshape(4 * rows, -1), False, *tools)

        return carried

    lax.fori_loop(0, steps, earlier, 0)

    broad_done[...] = jnp.transpose(acc[0:DB] / total[0]).astype(bf16).reshape(2, rows, DB)
    narrow_done[...] = (
        jnp.transpose(acc[DB : DB + DN] / total[1]).astype(bf16).reshape(2, rows, DN)
    )
    swap = [
        remote(broad_done.at[1 - core], broad_theirs, a_sems, 0, partner),
        remote(narrow_done.at[1 - core], narrow_theirs, a_sems, 1, partner),
    ]
    for copy in swap:
        copy.start()
    carry_out_until(clock + 1.5)
    for copy in swap:
        copy.wait_recv()
    pairs = [
        (mine, theirs[...])
        for mine, theirs in (
            (broad_done[core], broad_theirs),
            (narrow_done[core], narrow_theirs),
        )
    ]
    gathered[x] = jnp.concatenate(
        [half for mine, theirs in pairs for half in (
            jnp.where(core == 0, mine, theirs), jnp.where(core == 0, theirs, mine)
        )],
        axis=1,
    )
    halves = (pl.ds(0, rows // 2), pl.ds(rows // 2, rows // 2))

    def along_x(at, half, i, device):
        view = gathered.at[at, halves[half]]
        return remote(view, view, n_sems, i, device)

    around = [
        along_x(x, 0, 0, right),
        along_x(x, 1, 1, left),
        along_x(x, 1, 2, right),
        along_x(x, 0, 3, left),
        along_x(xs(x, -1), 0, 4, right),
        along_x(xs(x, 1), 1, 5, left),
    ]
    for copy in around[:4]:
        copy.start()
    spread.drain()
    carry_out_until(clock + 5.0)
    around[0].wait_recv()
    around[4].start()
    around[1].wait_recv()
    around[5].start()
    carry_out_until(clock + 9.0)
    for copy in around[2:]:
        copy.wait_recv()
    rows_broad = jnp.concatenate([gathered[i, :, 0 : 2 * DB] for i in range(parts)], axis=1)
    rows_narrow = jnp.concatenate(
        [gathered[i, :, 2 * DB : 2 * (DB + DN)] for i in range(parts)], axis=1
    )
    width = out.shape[1]

    def project(n, carried):
        columns = pl.ds(pl.multiple_of(n * CHUNK, CHUNK), CHUNK)
        wide[:, columns] = dot(rows_broad, out_broad[:, columns]) + dot(
            rows_narrow, out_narrow[:, columns]
        )
        return carried

    lax.fori_loop(0, width // CHUNK, project, 0)

    def norm_share(i, carried):
        at = pl.ds(pl.multiple_of(i * share, 16), share)
        mix = (resid[at].astype(f32) + rms_scale(wide[at], post_gain[...])).astype(bf16)
        mixed[i] = mix
        normed[i] = rms_scale(mix.astype(f32), ffn_gain[...]).astype(bf16)
        return carried

    lax.fori_loop(0, parts, norm_share, 0)
    inputs = normed[...].reshape(rows, width)
    carry_out_until(max(times["u", name] for name in w_tasks))

    def raise_up(n, carried):
        columns = pl.ds(pl.multiple_of(n * CHUNK, CHUNK), CHUNK)
        up = up_held[:, :, :, :, columns].reshape(width, CHUNK)
        raised = jnp.maximum(dot(inputs, up), 0.0)
        hidden[:, columns] = (raised * raised).astype(bf16)
        return carried

    lax.fori_loop(0, hidden.shape[1] // CHUNK, raise_up, 0)
    while lines:
        carry_out(lines.pop(0))

    pieces = width // CHUNK
    per_z = 2 * ny * model_rows
    copies = {}
    for n in range(pieces):
        d = 1 if n % 2 == 0 else -1
        columns = slice(n * CHUNK, (n + 1) * CHUNK)
        near, far = {"tp": xs(x, d)}, {"tp": xs(x, -d)}
        copies[n] = (
            remote(partial_sent.at[xs(x, 2), :, columns], relayed.at[n], r_sems, 3 * n, near),
            remote(
                partial_sent.at[xs(x, -d), :, columns],
                from_near.at[:, columns],
                r_sems,
                3 * n + 1,
                far,
            ),
            remote(combined.at[n], from_far.at[:, columns], r_sems, 3 * n + 2, near),
        )

    def lower(n):
        columns = slice(n * CHUNK, (n + 1) * CHUNK)
        zn = CHUNK // per_z
        down = down_held[n * zn : (n + 1) * zn].reshape(CHUNK, hidden.shape[1])
        sums = dot(hidden[...], down, LAST).reshape(parts, share, CHUNK)
        partial[:, :, columns] = sums
        partial_sent[:, :, columns] = sums.astype(bf16)
        copies[n][0].start()
        copies[n][1].start()

    def relay(n):
        d = 1 if n % 2 == 0 else -1
        columns = slice(n * CHUNK, (n + 1) * CHUNK)
        copies[n][0].wait_recv()
        combined[n] = (partial[xs(x, d), :, columns] + relayed[n].astype(f32)).astype(bf16)
        copies[n][2].start()

    for n in range(pieces):
        lower(n)
    for n in range(pieces):
        relay(n)
    up_web.drain()
    down_web.drain()
    for copy in exchange + swap + around:
        copy.wait_send()
    for n in range(pieces):
        copies[n][1].wait_recv()
        copies[n][2].wait_recv()
    ffn = partial[x] + from_near[...].astype(f32) + from_far[...].astype(f32)
    out[...] = (mixed[x].astype(f32) + rms_scale(ffn, ffn_out_gain[...])).astype(bf16)
    for n in range(pieces):
        for copy in copies[n]:
            copy.wait_send()


def rms_scale(values, norm_gain):
    return (
        values * lax.rsqrt(jnp.mean(values * values, axis=-1, keepdims=True) + norm_eps) * norm_gain
    )


def layer(geometry, latent, queries, tables, key_rope, ups, gains, resid, outs, up_weight, down_weight):
    nz, ny, parts = geometry
    rows, latent_width = latent.shape
    width = resid.shape[1]
    hidden = up_weight.shape[1]
    share = rows // parts
    model_rows = up_weight.shape[0]
    vmem = pl.BlockSpec(memory_space=pltpu.VMEM)
    anywhere = pl.BlockSpec(memory_space=pl.ANY)
    copies = len(copies_of(nz, ny, True)[0])
    w_copies = len(copies_of(nz, ny, False)[0])
    pieces = width // CHUNK
    sems = pltpu.SemaphoreType.DMA
    operands = (
        latent,
        *queries,
        *tables,
        key_rope,
        gains[0],
        *ups,
        *gains[1:],
        resid,
        *outs,
        up_weight,
        down_weight,
    )
    return pl.pallas_call(
        functools.partial(layer_kernel, geometry),
        out_shape=jax.ShapeDtypeStruct((share, width), bf16),
        in_specs=[anywhere] + [vmem] * 15 + [anywhere] * 5,
        out_specs=vmem,
        scratch_shapes=[
            pltpu.VMEM((nz, ny, 2, rows, latent_width + 128), bf16),
            pltpu.VMEM((nz, ny, 2, model_rows, hidden), bf16),
            pltpu.VMEM((nz, ny, 2, model_rows, hidden), bf16),
            pltpu.VMEM((2, rows, queries[0].shape[1]), bf16),
            pltpu.VMEM((2, rows, queries[1].shape[1]), bf16),
            pltpu.VMEM((256, 2 * rows), bf16),
            pltpu.VMEM((128, 2 * rows), bf16),
            pltpu.VMEM((512, 256), bf16),
            pltpu.VMEM((DB + DN, 512), bf16),
            pltpu.VMEM((2, 1, 2 * rows), f32),
            pltpu.VMEM((2, 1, 2 * rows), f32),
            pltpu.VMEM((DB + DN, 2 * rows), f32),
            pltpu.VMEM((rows // 2, latent_width), bf16),
            pltpu.VMEM((rows, 128), bf16),
            pltpu.VMEM((2, rows, DB), bf16),
            pltpu.VMEM((2, rows, DN), bf16),
            pltpu.VMEM((rows, DB), bf16),
            pltpu.VMEM((rows, DN), bf16),
            pltpu.VMEM((parts, rows, 2 * (DB + DN)), bf16),
            pltpu.VMEM(outs[0].shape, bf16),
            pltpu.VMEM(outs[1].shape, bf16),
            pltpu.VMEM((rows, width), bf16),
            pltpu.VMEM((rows, width), f32),
            pltpu.VMEM((parts, share, width), bf16),
            pltpu.VMEM((parts, share, width), bf16),
            pltpu.VMEM((rows, hidden), bf16),
            pltpu.VMEM((parts, share, width), f32),
            pltpu.VMEM((parts, share, width), bf16),
            pltpu.VMEM((pieces, share, CHUNK), bf16),
            pltpu.VMEM((pieces, share, CHUNK), bf16),
            pltpu.VMEM((share, width), bf16),
            pltpu.VMEM((share, width), bf16),
            sems((6,)),
            sems((copies,)),
            sems((copies,)),
            sems((w_copies,)),
            sems((w_copies,)),
            sems((w_copies,)),
            sems((w_copies,)),
            sems((2,)),
            sems((2,)),
            sems((2,)),
            sems((2,)),
            sems((6,)),
            sems((6,)),
            sems((3 * pieces,)),
            sems((3 * pieces,)),
        ],
        compiler_params=pltpu.CompilerParams(
            collective_id=0, has_side_effects=True, vmem_limit_bytes=63 * 1024 * 1024
        ),
        cost_estimate=pl.CostEstimate(
            flops=40_000_000_000, bytes_accessed=20_000_000, transcendentals=9_000_000
        ),
        name="layer",
    )(*operands)


def frequency_of(lane):
    return rope_base ** (-2.0 * lax.rem(lane, ROPE // 2).astype(f32) / ROPE)


def local(
    resid,
    query_broad,
    query_narrow,
    latent,
    key_rope,
    latent_gain,
    key_up_broad,
    value_up_broad,
    key_up_narrow,
    value_up_narrow,
    out_broad,
    out_narrow,
    post_gain,
    ffn_gain,
    up_weight,
    down_weight,
    ffn_out_gain,
):
    rows = resid.shape[0]
    parts = lax.axis_size("tp")
    me = lax.axis_index("sp")
    nz = lax.axis_size("sp") // (2 * NY)

    lane = jnp.arange(128, dtype=jnp.int32)
    positions = (me * rows + jnp.arange(rows, dtype=jnp.int32)).astype(f32)
    angles = positions[:, None] * frequency_of(lane)[None, :]
    sign = jnp.where(lane < ROPE, 0.0, jnp.where(lane < ROPE + ROPE // 2, -1.0, 1.0))
    key_cosines = jnp.cos(angles) * (sign * sign)[None, :]
    key_sines = jnp.sin(angles) * sign[None, :]
    lane = jnp.arange(ROPE, dtype=jnp.int32)
    positions = ((me // 2) * 2 * rows + jnp.arange(2 * rows, dtype=jnp.int32)).astype(f32)
    angles = frequency_of(lane)[:, None] * positions[None, :]
    cosines = jnp.cos(angles)
    sines = jnp.sin(angles) * jnp.where(lane < ROPE // 2, -1.0, 1.0)[:, None]
    return layer(
        (nz, NY, parts),
        latent,
        (query_broad, query_narrow),
        (cosines, sines, key_cosines, key_sines),
        key_rope.T,
        (key_up_broad, value_up_broad, key_up_narrow, value_up_narrow),
        (latent_gain[None, :], post_gain[None, :], ffn_gain[None, :], ffn_out_gain[None, :]),
        resid,
        (out_broad, out_narrow),
        up_weight,
        down_weight,
    )


def solution(mesh):
    in_specs = (
        P("sp", None),
        P("sp", "tp"),
        P("sp", "tp"),
        P("sp", None),
        P("sp", None),
        P(),
        P(None, "tp"),
        P(None, "tp"),
        P(None, "tp"),
        P(None, "tp"),
        P(),
        P(),
        P(),
        P(),
        P("sp", "tp"),
        P("sp", "tp"),
        P(),
    )
    out_specs = P(("sp", "tp"), None)
    return jax.shard_map(local, mesh=mesh, in_specs=in_specs, out_specs=out_specs, check_vma=False)
```
